128 devices in a mesh: fs: 16 (over z, y), tp: 8 (over x, core).
Axes of the slice: x: 4, y: 4, z: 4, core: 2. Of those that a mesh axis runs over, the one named last changes fastest.
Arguments:
- prompt: bfloat16 [8192, 4096], P('fs'), may hold values from -6 to 6
- expert_ids: int32 [8192, 2], P('fs'), may hold values from 0 to 31, all different within a row; in each aligned block of 512 rows (0 to 511, 512 to 1023, ...) at most 48 rows name the same one
- group_weight: float32 [8192], P('fs'), may hold values from 0.25 to 1
- expert_share: float32 [8192, 2], P('fs'), may hold values from 0.1 to 1
- norm_gain: float32 [4096], P('fs'), may hold values from 0.1 to 1.9
- gate_train: float32 [32, 4096, 1024], P(None, 'fs', 'tp'), may hold values from -0.09375 to 0.09375
- up_train: float32 [32, 4096, 1024], P(None, 'fs', 'tp'), may hold values from -0.09375 to 0.09375
- down_train: float32 [32, 1024, 4096], P(None, 'fs', 'tp'), may hold values from -0.1875 to 0.1875
Outputs:
- mixed: bfloat16 [8192, 4096], P('fs', 'tp')
- gate_new: bfloat16 [32, 4096, 1024], P('fs', None, 'tp')
- up_new: bfloat16 [32, 4096, 1024], P('fs', None, 'tp')
- down_new: bfloat16 [32, 1024, 4096], P('fs', 'tp')
The draws below stay inside these ranges and needn't reach their ends.
Inputs may be any that keep to these rules, and one draw needn't show every extreme that they name: `expert_ids`: each row names two different experts; within the rows of one index of fs no expert is named more than 48 times, a bound that some block reaches there.
All inputs are finite; a program needn't handle non-finite values.
Results may differ from the reference program's by a relative error of at most 0.0086.
Values may be sent and summed in bfloat16 or wider, within the bound.
A program may use at most 128 MiB of HBM per device.

```python
import math
import jax
import jax.numpy as jnp
import numpy as np
from jax import lax

D = 4096
FF = 1024
TOK_DEV = 512
EXPERTS = 32
TOKENS = 8192
CAP = 48
N_FS = 16


def levels(rng, extent, cuts, smallest, largest):
    gain = 1.0
    for position, shards_of in cuts:
        draws = jax.random.uniform(jax.random.fold_in(jax.random.fold_in(rng, 6), position), (shards_of,), jnp.float32, smallest / len(cuts), largest / len(cuts))
        gain = gain * jnp.repeat(jnp.exp(draws), extent[position] // shards_of).reshape((-1,) + (1,) * (len(extent) - 1 - position))
    return gain


def shared_out(rng, own, number, rows, count, top, most, skew):
    ranking = jax.random.permutation(rng, count)
    packed, ordinary = portions_of(count, rows * top, most, skew, True), portions_of(count, rows * top, most, skew, False)
    places = jnp.arange(count)

    def named(lengths, offset_by):
        used = int((lengths > 0).sum())
        fixed = max(1, used // 4)
        moved = fixed + (places - fixed + offset_by * (used - fixed)) % max(1, count - fixed)
        return jnp.zeros((count,), jnp.int32).at[ranking[jnp.where(places < fixed, places, moved)]].set(jnp.asarray(lengths, jnp.int32))

    lengths = jnp.where(number % 4 == 0, named(packed, number // 4), named(ordinary, number - number // 4 - 1))
    mixed = jax.random.permutation(jax.random.fold_in(own, 3), count)
    giver, sink = mixed[0:count // 2 * 2:2], mixed[1:count // 2 * 2:2]
    slack = jnp.minimum(lengths[giver] - 1, most - lengths[sink]) // 2
    slack = jnp.where((giver == ranking[0]) | (sink == ranking[0]) | (lengths[sink] == 0), 0, jnp.maximum(slack, 0))
    moved = jax.random.randint(jax.random.fold_in(own, 4), (count // 2,), 0, 1 << 20) % (slack + 1)
    lengths = lengths.at[giver].add(-moved).at[sink].add(moved)
    items = jnp.searchsorted(jnp.cumsum(lengths), jnp.arange(rows * top), side="right").astype(jnp.int32)
    grid = items.reshape(top, rows).T
    grid = grid[jax.random.permutation(jax.random.fold_in(own, 1), rows)]
    offset_by = jax.random.randint(jax.random.fold_in(own, 2), (rows, 1), 0, top)
    return jnp.take_along_axis(grid, (jnp.arange(top)[None, :] + offset_by) % top, axis=1)


def portions_of(count, total, reach, skew, full):
    portions = [(1 << 20) // math.isqrt(grade ** skew) + 1 for grade in range(1, count + 1)]
    largest = reach if full else min(reach, max(-(-total // count), total * portions[0] // sum(portions)))
    least = 1 if total - largest >= count - 1 else 0
    counts, spare = [largest] + [least] * (count - 1), total - largest - least * (count - 1)
    while spare > 0:
        candidates = [i for i in range(1, count) if counts[i] < largest] or [i for i in range(1, count) if counts[i] < reach]
        pool, remaining = sum([portions[i] for i in candidates]), spare
        for i in candidates:
            addition = min(reach - counts[i], max(1, remaining * portions[i] // pool), spare)
            counts[i] = counts[i] + addition
            spare = spare - addition
    return np.array(counts)


def bell_draw(rng, shape, spread, most, split=(), kind=jnp.bfloat16):
    array = spread * jax.random.normal(rng, shape, jnp.float32)
    if split:
        array = array * levels(rng, shape, split, -0.22, 0.18)
    return jnp.clip(array, -most, most).astype(kind)


def setup_inputs(seed: int = 0) -> dict:
    key_list = jax.random.split(jax.random.key(seed), 9)
    prompt = bell_draw(key_list[0], (TOKENS, D), 1.0, 6.0, ((0, 16),))
    expert_ids_keys = jax.random.split(jax.random.fold_in(key_list[1], 1), TOKENS // TOK_DEV)
    expert_ids_turns = jax.random.permutation(jax.random.fold_in(key_list[1], 3), TOKENS // TOK_DEV)
    expert_ids = jax.vmap(lambda own, number: shared_out(jax.random.fold_in(key_list[1], 2), own, number, TOK_DEV, EXPERTS, 2, CAP, 1))(expert_ids_keys, expert_ids_turns).reshape((TOKENS, 2))
    group_weight = jnp.clip(jnp.exp(math.log(1.0) - 1.3862944 * jax.random.uniform(key_list[2], (TOKENS,), jnp.float32) ** levels(key_list[2], (TOKENS,), ((0, 16),), -0.2, 0.2)), 0.25, 1.0)
    expert_share = jnp.clip(jnp.exp(math.log(1.0) - 2.3025851 * jax.random.uniform(key_list[3], (TOKENS, 2), jnp.float32) ** levels(key_list[3], (TOKENS, 2), ((0, 16),), -0.2, 0.2)), 0.1, 1.0)
    norm_gain = jnp.clip(1.0 + 0.18 * jax.random.normal(key_list[4], (D,), jnp.float32), 0.1, 1.9)
    gate_train = bell_draw(key_list[5], (EXPERTS, D, FF), D ** -0.5, 0.09375, ((1, 16), (2, 8)), jnp.float32)
    up_train = bell_draw(key_list[6], (EXPERTS, D, FF), D ** -0.5, 0.09375, ((1, 16), (2, 8)), jnp.float32)
    down_train = bell_draw(key_list[7], (EXPERTS, FF, D), FF ** -0.5, 0.1875, ((1, 16), (2, 8)), jnp.float32)
    return dict(prompt=prompt, expert_ids=expert_ids, group_weight=group_weight, expert_share=expert_share, norm_gain=norm_gain, gate_train=gate_train, up_train=up_train, down_train=down_train)


EPS = 1e-06

def reference(prompt, expert_ids, group_weight, expert_share, norm_gain, gate_train, up_train, down_train):
    gain_rows = norm_gain[None, :, None]
    gate_new = (gate_train * gain_rows).astype(jnp.bfloat16)
    up_new = (up_train * gain_rows).astype(jnp.bfloat16)
    down_new = down_train.astype(jnp.bfloat16)
    widened = prompt.astype(jnp.float32)
    normed = (widened * lax.rsqrt(lax.optimization_barrier(jnp.mean(widened * widened, axis=-1, keepdims=True)) + EPS)).astype(jnp.bfloat16)
    blocks = expert_ids.reshape(N_FS, TOK_DEV * 2)
    onehot = (blocks[:, :, None] == jnp.arange(EXPERTS, dtype=jnp.int32)[None, None, :]).astype(jnp.int32)
    slot_rank = lax.optimization_barrier(jnp.sum((jnp.cumsum(onehot, axis=1) - 1) * onehot, axis=2))
    slots = (jnp.arange(N_FS, dtype=jnp.int32)[:, None] * CAP + slot_rank).reshape(TOKENS, 2).astype(jnp.int32)
    token_rows = jnp.broadcast_to(normed[:, None, :], (TOKENS, 2, D))
    buffer = jnp.zeros((EXPERTS, N_FS * CAP, D), jnp.bfloat16).at[expert_ids, slots].set(token_rows)

    def expert(operands):
        expert_rows, w_gate, w_up, w_down = operands
        gate_val = jnp.dot(expert_rows, w_gate, preferred_element_type=jnp.float32)
        up_val = jnp.dot(expert_rows, w_up, preferred_element_type=jnp.float32)
        hidden = (jax.nn.silu(gate_val) * up_val).astype(jnp.bfloat16)
        return jnp.dot(hidden, w_down, preferred_element_type=jnp.float32).astype(jnp.bfloat16)
    outputs = lax.map(expert, (buffer, gate_new, up_new, down_new))
    picked = outputs[expert_ids, slots].astype(jnp.float32)
    weights = group_weight[:, None] * expert_share / lax.optimization_barrier(jnp.sum(expert_share, axis=1, keepdims=True))
    mixed = lax.optimization_barrier(jnp.sum(weights[:, :, None] * picked, axis=1)).astype(jnp.bfloat16)
    return (mixed, gate_new, up_new, down_new)
```

```python
import jax
import jax.numpy as jnp
from jax import lax
from jax.experimental import pallas as pl
from jax.experimental.pallas import tpu as pltpu
from jax.sharding import PartitionSpec as P

MESH = pl.DeviceIdType.MESH
BF = jnp.bfloat16
F32 = jnp.float32
EPS = 1e-06
CAP = 48
EARLY = (1, 3, 4, 12)
LATE = (2, 5, 6, 7, 8, 9, 10, 11, 13, 14, 15)


def kernel(
    prompt, ids, gw, share, gain, gate, up, down,
    mixed_o, gate_o, up_o, down_o,
    pf, po, xn, gb, sg, su, sd, wsend, dsend, cm, pick, tsend, rows, wrecv, drecv, acc,
    hid, osend, ret, cols, comb, dnew,
    l_p, l_g, l_u, l_d, t_s, t_r, w_s, w_r, x_s, x_r, h_s, h_r, d_s, d_r, n_s, n_r, b_s, b_r, o_s,
):
    f = lax.axis_index("fs")
    t = lax.axis_index("tp")
    z, y = f // 4, f % 4
    x, c = t // 2, t % 2
    right = ((x + 1) % 4) * 2 + c
    left = ((x + 3) % 4) * 2 + c
    across = ((x + 2) % 4) * 2 + c
    mate = x * 2 + 1 - c
    flip = 1 - 2 * c

    def to(k):
        return ((z + k // 4) % 4) * 4 + (y + k % 4) % 4

    def came(k):
        return ((z + 4 - k // 4) % 4) * 4 + (y + 4 - k % 4) % 4

    def at(start, size, unit):
        return pl.ds(pl.multiple_of(start, unit), size)

    def local(src, dst, sem):
        return pltpu.make_async_copy(src, dst, sem)

    def remote(src, dst, ssem, rsem, fs, tp):
        return pltpu.make_async_remote_copy(
            src_ref=src, dst_ref=dst, send_sem=ssem, recv_sem=rsem,
            device_id=(fs, tp), device_id_type=MESH,
        )

    def load_prompt(i):
        return local(prompt.at[pl.ds(i * 128, 128), :], pf.at[pl.ds(i * 128, 128), :], l_p.at[i])

    def load_own():
        return local(prompt.at[:, at(t * 512, 512, 512)], po, l_p.at[4])

    def load_gate(k):
        return local(gate.at[to(k)], sg.at[k], l_g.at[k])

    def load_up(k):
        return local(up.at[to(k)], su.at[k], l_u.at[k])

    def load_down(k, slot):
        return local(down.at[to(k)], sd.at[slot], l_d.at[slot])

    for k in EARLY:
        load_gate(k).start()
        load_up(k).start()
    load_own().start()
    for i in range(4):
        load_prompt(i).start()

    barrier = pltpu.get_barrier_semaphore()

    def greet_fs(k, carry):
        pl.semaphore_signal(barrier, inc=1, device_id=(to(k), t), device_id_type=MESH)
        return carry

    def greet_tp(k, carry):
        pl.semaphore_signal(barrier, inc=1, device_id=(f, (t + k) % 8), device_id_type=MESH)
        return carry

    lax.fori_loop(1, 16, greet_fs, 0)
    lax.fori_loop(1, 8, greet_tp, 0)

    for k in (0,) + LATE:
        load_gate(k).start()
        load_up(k).start()
    for k in range(8):
        load_down(k, k).start()

    gb[...] = jnp.broadcast_to(gain[...], (128, 256)).T

    def cast_weights(k):
        load_gate(k).wait()
        load_up(k).wait()
        for e in range(2):
            wsend[k, e, 0] = (sg[k, e] * gb[...]).astype(BF)
            wsend[k, e, 1] = (su[k, e] * gb[...]).astype(BF)

    def weights_copy(k):
        return remote(
            wsend.at[k], wrecv.at[:, :, at(f * 256, 256, 256), :], w_s.at[k], w_r.at[k], to(k), t
        )

    for k in EARLY:
        cast_weights(k)
    pl.semaphore_wait(barrier, 22)
    for k in EARLY:
        weights_copy(k).start()

    def rank_slots():
        expert = lax.broadcasted_iota(jnp.int32, (32, 512), 0)
        hit0 = ids[0:1, :] == expert
        hit1 = ids[1:2, :] == expert
        named = jnp.where(hit0 | hit1, 1.0, 0.0)
        before = jnp.where(
            lax.broadcasted_iota(jnp.int32, (512, 512), 0)
            < lax.broadcasted_iota(jnp.int32, (512, 512), 1), 1.0, 0.0,
        ).astype(BF)
        count = jnp.dot(named.astype(BF), before, preferred_element_type=F32)
        cm[...] = jnp.where(named > 0.5, count, -1.0)
        total = share[0:1, :] + share[1:2, :]
        for k, hit in ((0, hit0), (1, hit1)):
            rank = jnp.sum(jnp.where(hit, count, 0.0), axis=0, keepdims=True)
            cols[k : k + 1, :] = ids[k : k + 1, :].astype(F32) * float(CAP) + rank
            cols[k + 2 : k + 3, :] = gw[...] * share[k : k + 1, :] / total

    cols[...] = jnp.zeros_like(cols)
    rank_slots()

    def build_pick(e, carry):
        slot = lax.broadcasted_iota(jnp.int32, (CAP, 512), 0).astype(F32)
        pick[e] = jnp.where(cm[pl.ds(e, 1), :] == slot, 1.0, 0.0).astype(BF)
        return carry

    lax.fori_loop(0, 32, build_pick, 0)

    load_own().wait()
    for i in range(4):
        load_prompt(i).wait()

    def normalize(i, carry):
        block = at(i * 32, 32, 32)
        squares = jnp.zeros((32, 128), F32)
        for j in range(32):
            part = pf[block, j * 128 : (j + 1) * 128].astype(F32)
            squares = squares + part * part
        mean = jnp.sum(squares, axis=1, keepdims=True) * (1.0 / 4096.0)
        xn[block, :] = (po[block, :].astype(F32) * lax.rsqrt(mean + EPS)).astype(BF)
        return carry

    lax.fori_loop(0, 16, normalize, 0)

    def token_copy(k):
        return remote(
            tsend.at[k // 4, (y + k % 4) % 4],
            rows.at[t, :, at(f * CAP, CAP, CAP), :],
            t_s.at[k], t_r.at[k], to(k), t,
        )

    for g in range(4):
        chosen = pick[pl.ds(((z + g) % 4) * 8, 8)].reshape(384, 512)
        tsend[g] = (
            jnp.dot(chosen, xn[...], preferred_element_type=F32).astype(BF).reshape(4, 2, CAP, 512)
        )
        for gy in range(4):
            if g + gy:
                token_copy(4 * g + gy).start()
    rows[t, :, at(f * CAP, CAP, CAP), :] = tsend[0, y]

    for k in LATE:
        cast_weights(k)
        weights_copy(k).start()
    cast_weights(0)
    wrecv[:, :, at(f * 256, 256, 256), :] = wsend[0]

    def block_rows(g):
        return at(((z + 4 - g) % 4) * 192, 192, 192)

    def row_copy(g, n):
        r = block_rows(g)
        both = {0: (t, right), 1: (t, left), 2: (t, mate), 3: (left, mate), 5: (right, mate)}
        if n in both:
            s, who = both[n]
            ref = rows.at[s, :, r, :]
        else:
            s, e, who = {4: (left, 0, right), 6: (right, 1, left), 7: (across, 0, mate), 8: (across, 1, mate)}[n]
            ref = rows.at[s, e, r, :]
        return remote(ref, ref, x_s.at[g, n], x_r.at[g, n], f, who)

    def row_arrival(g, n):
        r = block_rows(g)
        both = {0: left, 1: right, 2: mate, 3: left + flip, 5: right + flip}
        if n in both:
            ref = rows.at[both[n], :, r, :]
        else:
            s, e = {4: (across, 0), 6: (across, 1), 7: (across + flip, 0), 8: (across + flip, 1)}[n]
            ref = rows.at[s, e, r, :]
        return remote(ref, ref, x_s.at[g, n], x_r.at[g, n], f, mate)

    def token_arrival(k):
        ref = rows.at[t, :, at(came(k) * CAP, CAP, CAP), :]
        return remote(tsend.at[0, 0], ref, t_s.at[k], t_r.at[k], f, mate)

    for g in range(4):
        for gy in range(4):
            if g + gy:
                token_arrival(4 * g + gy).wait_recv()
        for n in range(3):
            row_copy(g, n).start()

    def down_copy(k):
        return remote(
            dsend.at[k], drecv.at[:, at(f * 64, 64, 64), :], d_s.at[k], d_r.at[k], to(k), t
        )

    def relay(g):
        row_arrival(g, 0).wait_recv()
        row_copy(g, 3).start()
        row_copy(g, 4).start()
        row_arrival(g, 1).wait_recv()
        row_copy(g, 5).start()
        row_copy(g, 6).start()

    def cast_down(k, slot):
        load_down(k, slot).wait()
        for e in range(2):
            dsend[k, e] = sd[slot, e].astype(BF)

    relay(0)
    for k in range(8):
        cast_down(k, k)
    for k in range(8, 16):
        load_down(k, k - 8).start()
    relay(1)
    for k in range(8, 16):
        cast_down(k, k - 8)
    drecv[:, at(f * 64, 64, 64), :] = dsend[0]
    relay(2)
    for k in range(1, 16):
        down_copy(k).start()
    cols_t = cols[...].T
    lane = lax.broadcasted_iota(jnp.int32, (512, 1536), 1).astype(F32)
    for k in range(2):
        comb[k] = jnp.where(cols_t[:, k : k + 1] == lane, 1.0, 0.0).astype(BF)
    relay(3)
    for g in range(4):
        row_arrival(g, 4).wait_recv()
        row_copy(g, 7).start()
        row_arrival(g, 6).wait_recv()
        row_copy(g, 8).start()

    def weights_arrival(k):
        ref = wrecv.at[:, :, at(came(k) * 256, 256, 256), :]
        return remote(wsend.at[k], ref, w_s.at[k], w_r.at[k], f, mate)

    for k in range(1, 16):
        weights_arrival(k).wait_recv()
    gate_out = local(wrecv.at[:, 0], gate_o, o_s.at[0])
    up_out = local(wrecv.at[:, 1], up_o, o_s.at[1])
    gate_out.start()
    up_out.start()
    for g in range(4):
        for n in (2, 3, 5, 7, 8):
            row_arrival(g, n).wait_recv()

    def hidden_copy(n):
        s, e, who = (
            (t, 0, right), (t, 1, right), (t, 1, left), (t, 0, left), (t, 0, mate), (t, 1, mate),
            (left, 0, mate), (left, 0, right), (left, 1, mate), (right, 1, mate), (right, 1, left),
            (right, 0, mate), (across, 0, mate), (across, 1, mate),
        )[n]
        ref = hid.at[s, e]
        return remote(ref, ref, h_s.at[n], h_r.at[n], f, who)

    def hidden_arrival(n):
        s, e = (
            (left, 0), (left, 1), (right, 1), (right, 0), (mate, 0), (mate, 1),
            (left + flip, 0), (across, 0), (left + flip, 1), (right + flip, 1), (across, 1),
            (right + flip, 0), (across + flip, 0), (across + flip, 1),
        )[n]
        ref = hid.at[s, e]
        return remote(ref, ref, h_s.at[n], h_r.at[n], f, mate)

    acc[...] = jnp.zeros_like(acc)
    for e in range(2):

        def project(s, carry):
            part = at(s * 512, 512, 512)
            both = jnp.concatenate([wrecv[e, 0, part, :], wrecv[e, 1, part, :]], axis=1)
            acc[e] += jnp.dot(rows[s, e], both, preferred_element_type=F32)
            return carry

        lax.fori_loop(0, 8, project, 0)
        v = acc[e, :, 0:128]
        hid[t, e] = (v / (1.0 + jnp.exp(-v)) * acc[e, :, 128:256]).astype(BF)

    for n in range(6):
        hidden_copy(n).start()
    for n, onward in ((0, (6, 7)), (2, (9, 10)), (1, (8,)), (3, (11,)), (7, (12,)), (10, (13,))):
        hidden_arrival(n).wait_recv()
        for m in onward:
            hidden_copy(m).start()

    def down_arrival(k):
        ref = drecv.at[:, at(came(k) * 64, 64, 64), :]
        return remote(dsend.at[k], ref, d_s.at[k], d_r.at[k], f, mate)

    for k in range(1, 16):
        down_arrival(k).wait_recv()
    for n in (4, 5, 6, 8, 9, 11, 12, 13):
        hidden_arrival(n).wait_recv()

    def new_copy(k):
        s = (t + k) % 8
        return remote(
            drecv.at[:, at(s * 128, 128, 128), :], dnew.at[t], n_s.at[k], n_r.at[k], f, s
        )

    def back_copy(k):
        return remote(
            osend.at[k // 4, :, at(((y + k % 4) % 4) * CAP, CAP, CAP), :],
            ret.at[pl.ds(2 * f, 2)], b_s.at[k], b_r.at[k], to(k), t,
        )

    for g in range(4):
        part = at(((z + g) % 4) * 192, 192, 192)
        for e in range(2):
            h = jnp.concatenate([hid[s, e, part, :] for s in range(8)], axis=1)
            osend[g, e] = jnp.dot(h, drecv[e], preferred_element_type=F32).astype(BF)
        for gy in range(4):
            if g + gy:
                back_copy(4 * g + gy).start()
    ret[pl.ds(2 * f, 2)] = osend[0, :, at(y * CAP, CAP, CAP), :]
    for k in range(1, 8):
        new_copy(k).start()
    dnew[t] = drecv[:, at(t * 128, 128, 128), :]

    def new_out(s):
        return local(dnew.at[s], down_o.at[:, :, pl.ds(s * 512, 512)], o_s.at[2 + s])

    def new_arrival(k):
        return remote(
            drecv.at[:, pl.ds(0, 128), :], dnew.at[(t + 8 - k) % 8], n_s.at[k], n_r.at[k], f, mate
        )

    def back_arrival(k):
        return remote(
            osend.at[0, :, pl.ds(0, CAP), :], ret.at[pl.ds(2 * came(k), 2)], b_s.at[k], b_r.at[k], f, mate
        )

    for k in range(1, 16):
        back_arrival(k).wait_recv()
    w_t = cols[...].T
    back = ret[...].reshape(1536, 512)
    first = jnp.dot(comb[0], back, preferred_element_type=F32) * w_t[:, 2:3]
    second = jnp.dot(comb[1], back, preferred_element_type=F32) * w_t[:, 3:4]
    mixed_o[...] = (first + second).astype(BF)

    for k in range(1, 8):
        new_arrival(k).wait_recv()
    for s in range(8):
        new_out(s).start()

    for k in range(1, 16):
        token_copy(k).wait_send()
        weights_copy(k).wait_send()
        down_copy(k).wait_send()
        back_copy(k).wait_send()
    for g in range(4):
        for n in range(9):
            row_copy(g, n).wait_send()
    for n in range(14):
        hidden_copy(n).wait_send()
    for k in range(1, 8):
        new_copy(k).wait_send()
    gate_out.wait()
    up_out.wait()
    for s in range(8):
        new_out(s).wait()


def on_device(
    prompt, expert_ids, group_weight, expert_share, norm_gain, gate_train, up_train, down_train
):
    any_ref = pl.BlockSpec(memory_space=pl.ANY)
    vmem_ref = pl.BlockSpec(memory_space=pltpu.VMEM)
    dma = pltpu.SemaphoreType.DMA
    return pl.pallas_call(
        kernel,
        out_shape=(
            jax.ShapeDtypeStruct((512, 512), BF),
            jax.ShapeDtypeStruct((2, 4096, 128), BF),
            jax.ShapeDtypeStruct((2, 4096, 128), BF),
            jax.ShapeDtypeStruct((2, 128, 4096), BF),
        ),
        in_specs=[any_ref, vmem_ref, vmem_ref, vmem_ref, vmem_ref, any_ref, any_ref, any_ref],
        out_specs=(vmem_ref, any_ref, any_ref, any_ref),
        scratch_shapes=[
            pltpu.VMEM((512, 4096), BF),
            pltpu.VMEM((512, 512), BF),
            pltpu.VMEM((512, 512), BF),
            pltpu.VMEM((256, 128), F32),
            pltpu.VMEM((16, 2, 256, 128), F32),
            pltpu.VMEM((16, 2, 256, 128), F32),
            pltpu.VMEM((8, 2, 64, 512), F32),
            pltpu.VMEM((16, 2, 2, 256, 128), BF),
            pltpu.VMEM((16, 2, 64, 512), BF),
            pltpu.VMEM((32, 512), F32),
            pltpu.VMEM((32, CAP, 512), BF),
            pltpu.VMEM((4, 4, 2, CAP, 512), BF),
            pltpu.VMEM((8, 2, 768, 512), BF),
            pltpu.VMEM((2, 2, 4096, 128), BF),
            pltpu.VMEM((2, 1024, 512), BF),
            pltpu.VMEM((2, 768, 256), F32),
            pltpu.VMEM((8, 2, 768, 128), BF),
            pltpu.VMEM((4, 2, 192, 512), BF),
            pltpu.VMEM((32, CAP, 512), BF),
            pltpu.VMEM((128, 512), F32),
            pltpu.VMEM((2, 512, 1536), BF),
            pltpu.VMEM((8, 2, 128, 512), BF),
            dma((5,)), dma((16,)), dma((16,)), dma((8,)),
            dma((16,)), dma((16,)), dma((16,)), dma((16,)),
            dma((4, 9)), dma((4, 9)), dma((14,)), dma((14,)),
            dma((16,)), dma((16,)), dma((8,)), dma((8,)),
            dma((16,)), dma((16,)), dma((10,)),
        ],
        compiler_params=pltpu.CompilerParams(
            collective_id=0, has_side_effects=True, vmem_limit_bytes=67043328
        ),
        name="handover",
    )(
        prompt,
        expert_ids.T,
        group_weight.reshape(1, -1),
        expert_share.T,
        norm_gain.reshape(1, -1),
        gate_train.reshape(16, 2, 256, 128),
        up_train.reshape(16, 2, 256, 128),
        down_train.reshape(16, 2, 64, 512),
    )


def solution(mesh):
    placed = (
        P("fs", None),
        P("fs", None),
        P("fs"),
        P("fs", None),
        P("fs"),
        P(None, "fs", "tp"),
        P(None, "fs", "tp"),
        P(None, "fs", "tp"),
    )
    return jax.shard_map(
        on_device,
        mesh=mesh,
        in_specs=placed,
        out_specs=(P("fs", "tp"), P("fs", None, "tp"), P("fs", None, "tp"), P("fs", "tp", None)),
        check_vma=False,
    )
```

```python
import jax
import jax.numpy as jnp
from jax import lax
from jax.experimental import pallas as pl
from jax.experimental.pallas import tpu as pltpu
from jax.sharding import PartitionSpec as P

MESH = pl.DeviceIdType.MESH
BF = jnp.bfloat16
F32 = jnp.float32
EPS = 1e-06
CAP = 48
ORDER = (4, 12, 1, 3, 5, 15, 7, 13, 8, 2, 10, 6, 14, 9, 11)


def kernel(
    prompt, ids, gw, share, gain, gate, up, down,
    mixed_o, gate_o, up_o, down_o,
    pf, po, xn, gb, sg, su, sd, wsend, dsend, cm, pick, tsend, rows, wrecv, drecv, acc,
    hid, osend, ret, cols, comb, macc, dnew,
    l_p, l_g, l_u, l_d, t_s, t_r, w_s, w_r, x_s, x_r, h_s, h_r, d_s, d_r, n_s, n_r, b_s, b_r, o_s,
):
    f = lax.axis_index("fs")
    t = lax.axis_index("tp")
    z, y = f // 4, f % 4
    x, c = t // 2, t % 2
    right = ((x + 1) % 4) * 2 + c
    left = ((x + 3) % 4) * 2 + c
    across = ((x + 2) % 4) * 2 + c
    mate = x * 2 + 1 - c
    flip = 1 - 2 * c

    def to(k):
        return ((z + k // 4) % 4) * 4 + (y + k % 4) % 4

    def came(k):
        return ((z + 4 - k // 4) % 4) * 4 + (y + 4 - k % 4) % 4

    def at(start, size, unit):
        return pl.ds(pl.multiple_of(start, unit), size)

    def local(src, dst, sem):
        return pltpu.make_async_copy(src, dst, sem)

    def remote(src, dst, ssem, rsem, fs, tp):
        return pltpu.make_async_remote_copy(
            src_ref=src, dst_ref=dst, send_sem=ssem, recv_sem=rsem,
            device_id=(fs, tp), device_id_type=MESH,
        )

    def load_prompt(i):
        return local(prompt.at[pl.ds(i * 128, 128), :], pf.at[pl.ds(i * 128, 128), :], l_p.at[i])

    def load_own():
        return local(prompt.at[:, at(t * 512, 512, 512)], po, l_p.at[4])

    def load_gate(k):
        return local(gate.at[to(k)], sg.at[k], l_g.at[k])

    def load_up(k):
        return local(up.at[to(k)], su.at[k], l_u.at[k])

    def load_down(k, slot):
        return local(down.at[to(k)], sd.at[slot], l_d.at[slot])

    load_own().start()
    for i in range(4):
        load_prompt(i).start()

    barrier = pltpu.get_barrier_semaphore()

    def greet_fs(k, carry):
        pl.semaphore_signal(barrier, inc=1, device_id=(to(k), t), device_id_type=MESH)
        return carry

    def greet_tp(k, carry):
        pl.semaphore_signal(barrier, inc=1, device_id=(f, (t + k) % 8), device_id_type=MESH)
        return carry

    lax.fori_loop(1, 16, greet_fs, 0)
    lax.fori_loop(1, 8, greet_tp, 0)

    for k in ORDER + (0,):
        load_gate(k).start()
        load_up(k).start()
    for k in range(8):
        load_down(k, k).start()

    gb[...] = jnp.broadcast_to(gain[...], (128, 256)).T

    def rank_slots():
        expert = lax.broadcasted_iota(jnp.int32, (32, 512), 0)
        hit0 = ids[0:1, :] == expert
        hit1 = ids[1:2, :] == expert
        named = jnp.where(hit0 | hit1, 1.0, 0.0)
        before = jnp.where(
            lax.broadcasted_iota(jnp.int32, (512, 512), 0)
            < lax.broadcasted_iota(jnp.int32, (512, 512), 1), 1.0, 0.0,
        ).astype(BF)
        count = jnp.dot(named.astype(BF), before, preferred_element_type=F32)
        cm[...] = jnp.where(named > 0.5, count, -1.0)
        total = share[0:1, :] + share[1:2, :]
        for k, hit in ((0, hit0), (1, hit1)):
            rank = jnp.sum(jnp.where(hit, count, 0.0), axis=0, keepdims=True)
            expert_of = ids[k : k + 1, :]
            place = (expert_of & 1) * 768 + (expert_of >> 1) * CAP
            cols[k : k + 1, :] = place.astype(F32) + rank
            cols[k + 2 : k + 3, :] = gw[...] * share[k : k + 1, :] / total

    cols[...] = jnp.zeros_like(cols)
    rank_slots()

    def build_pick(e, carry):
        slot = lax.broadcasted_iota(jnp.int32, (CAP, 512), 0).astype(F32)
        pick[e] = jnp.where(cm[pl.ds(e, 1), :] == slot, 1.0, 0.0).astype(BF)
        return carry

    lax.fori_loop(0, 32, build_pick, 0)

    load_own().wait()
    for i in range(4):
        load_prompt(i).wait()

    def normalize(i, carry):
        block = at(i * 32, 32, 32)
        squares = jnp.zeros((32, 128), F32)
        for j in range(32):
            part = pf[block, j * 128 : (j + 1) * 128].astype(F32)
            squares = squares + part * part
        mean = jnp.sum(squares, axis=1, keepdims=True) * (1.0 / 4096.0)
        xn[block, :] = (po[block, :].astype(F32) * lax.rsqrt(mean + EPS)).astype(BF)
        return carry

    lax.fori_loop(0, 16, normalize, 0, unroll=4)

    for g in range(4):
        chosen = pick[g * 8 : g * 8 + 8].reshape(384, 512)
        tsend[4 * g : 4 * g + 4] = (
            jnp.dot(chosen, xn[...], preferred_element_type=F32).astype(BF).reshape(4, 2, CAP, 512)
        )

    def token_copy(k):
        return remote(
            tsend.at[to(k)], rows.at[t, :, at(f * CAP, CAP, CAP), :],
            t_s.at[k], t_r.at[k], to(k), t,
        )

    pl.semaphore_wait(barrier, 22)
    for k in ORDER:
        token_copy(k).start()
    rows[t, :, at(f * CAP, CAP, CAP), :] = tsend[f]

    def cast_weights(k, e):
        wsend[k, e, 0] = (sg[k, e] * gb[...]).astype(BF)
        wsend[k, e, 1] = (su[k, e] * gb[...]).astype(BF)

    def weights_copy(k, e, m):
        return remote(
            wsend.at[k, e, m], wrecv.at[e, m, at(f * 256, 256, 256), :],
            w_s.at[e, k], w_r.at[e, k], to(k), t,
        )

    def weights_pair(k, e):
        return remote(
            wsend.at[k, e], wrecv.at[e, :, at(came(k) * 256, 256, 256), :],
            w_s.at[e, k], w_r.at[e, k], to(k), t,
        )

    for k in ORDER + (0,):
        load_gate(k).wait()
        load_up(k).wait()
        cast_weights(k, 0)
    for m in range(2):
        for k in ORDER:
            weights_copy(k, 0, m).start()
    for k in ORDER + (0,):
        cast_weights(k, 1)
    wrecv[:, :, at(f * 256, 256, 256), :] = wsend[0]
    for m in range(2):
        for k in ORDER:
            weights_copy(k, 1, m).start()

    def row_copy(k, n):
        r = at(came(k) * CAP, CAP, CAP)
        both = {0: (t, right), 1: (t, left), 2: (t, mate), 3: (left, mate), 5: (right, mate)}
        if n in both:
            s, who = both[n]
            ref = rows.at[s, :, r, :]
        else:
            s, e, who = {4: (left, 0, right), 6: (right, 1, left), 7: (across, 0, mate), 8: (across, 1, mate)}[n]
            ref = rows.at[s, e, r, :]
        return remote(ref, ref, x_s.at[k, n], x_r.at[k, n], f, who)

    def row_arrival(k, n):
        r = at(came(k) * CAP, CAP, CAP)
        both = {0: left, 1: right, 2: mate, 3: left + flip, 5: right + flip}
        if n in both:
            ref = rows.at[both[n], :, r, :]
        else:
            s, e = {4: (across, 0), 6: (across, 1), 7: (across + flip, 0), 8: (across + flip, 1)}[n]
            ref = rows.at[s, e, r, :]
        return remote(ref, ref, x_s.at[k, n], x_r.at[k, n], f, mate)

    def token_arrival(k):
        ref = rows.at[t, :, at(came(k) * CAP, CAP, CAP), :]
        return remote(tsend.at[0], ref, t_s.at[k], t_r.at[k], f, mate)

    for k in (0,) + ORDER:
        if k:
            token_arrival(k).wait_recv()
        for n in range(3):
            row_copy(k, n).start()

    def down_copy(k, e):
        return remote(
            dsend.at[k, e], drecv.at[e, at(f * 64, 64, 64), :], d_s.at[e, k], d_r.at[e, k], to(k), t
        )

    def cast_down(k, slot):
        load_down(k, slot).wait()
        for e in range(2):
            dsend[k, e] = sd[slot, e].astype(BF)

    def relay(k):
        row_arrival(k, 0).wait_recv()
        row_copy(k, 4).start()
        row_copy(k, 3).start()
        row_arrival(k, 1).wait_recv()
        row_copy(k, 6).start()
        row_copy(k, 5).start()

    for k in range(8):
        cast_down(k, k)
    for k in range(8, 16):
        load_down(k, k - 8).start()
    chain = (0,) + ORDER
    for k in chain[:6]:
        relay(k)
    for k in range(8, 16):
        cast_down(k, k - 8)
    drecv[:, at(f * 64, 64, 64), :] = dsend[0]
    for e in range(2):
        for k in ORDER:
            down_copy(k, e).start()
    for k in chain[6:11]:
        relay(k)
    cols_t = cols[...].T
    lane = lax.broadcasted_iota(jnp.int32, (512, 768), 1).astype(F32)
    for k in range(2):
        for e in range(2):
            comb[k, e] = jnp.where(cols_t[:, k : k + 1] == lane + 768.0 * e, 1.0, 0.0).astype(BF)
    for k in chain[11:]:
        relay(k)

    def project(e, chip):
        part = at(chip * 1024, 1024, 1024)
        left_side = jnp.concatenate([rows[2 * chip, e], rows[2 * chip + 1, e]], axis=1)
        both = jnp.concatenate([wrecv[e, 0, part, :], wrecv[e, 1, part, :]], axis=1)
        return jnp.dot(left_side, both, preferred_element_type=F32)

    def near(e):
        acc[e] = project(e, x)

        def step(j, carry):
            acc[e] += project(e, (x + j + j // 2) % 4)
            return carry

        lax.fori_loop(1, 3, step, 0)

    def finish(e):
        acc[e] += project(e, (x + 2) % 4)
        v = acc[e, :, 0:128]
        hid[t, e] = (v / (1.0 + jnp.exp(-v)) * acc[e, :, 128:256]).astype(BF)

    def hidden_ref(s, e, part):
        return hid.at[s, e] if part is None else hid.at[s, e, pl.ds(part * 384, 384), :]

    def hidden_copy(e, n):
        s, part, who = (
            (t, None, right), (t, None, left), (t, None, mate), (left, None, mate), (left, 0, right),
            (right, None, mate), (right, 1, left), (across, 0, mate), (across, 1, mate),
        )[n]
        ref = hidden_ref(s, e, part)
        return remote(ref, ref, h_s.at[e, n], h_r.at[e, n], f, who)

    def hidden_arrival(e, n):
        s, part = (
            (left, None), (right, None), (mate, None), (left + flip, None), (across, 0),
            (right + flip, None), (across, 1), (across + flip, 0), (across + flip, 1),
        )[n]
        ref = hidden_ref(s, e, part)
        return remote(ref, ref, h_s.at[e, n], h_r.at[e, n], f, mate)

    for k in ORDER:
        weights_pair(k, 0).wait_recv()
    for k in chain:
        for n in (2, 3, 5):
            row_arrival(k, n).wait_recv()
    near(0)
    for k in chain:
        row_arrival(k, 4).wait_recv()
        row_copy(k, 7).start()
        row_arrival(k, 6).wait_recv()
        row_copy(k, 8).start()
    for k in chain:
        for n in (7, 8):
            row_arrival(k, n).wait_recv()
    finish(0)
    for n in range(3):
        hidden_copy(0, n).start()
    for k in ORDER:
        weights_pair(k, 1).wait_recv()
    gate_out = local(wrecv.at[:, 0], gate_o, o_s.at[0])
    up_out = local(wrecv.at[:, 1], up_o, o_s.at[1])
    near(1)
    finish(1)
    for n in range(3):
        hidden_copy(1, n).start()
    gate_out.start()
    up_out.start()

    for e in range(2):
        hidden_arrival(e, 0).wait_recv()
        hidden_copy(e, 4).start()
        hidden_copy(e, 3).start()
        hidden_arrival(e, 1).wait_recv()
        hidden_copy(e, 6).start()
        hidden_copy(e, 5).start()

    def down_arrival(k, e):
        ref = drecv.at[e, at(came(k) * 64, 64, 64), :]
        return remote(dsend.at[k, e], ref, d_s.at[e, k], d_r.at[e, k], f, mate)

    def new_copy(k, e):
        s = (t + k) % 8
        return remote(
            drecv.at[e, at(s * 128, 128, 128), :], dnew.at[t, e], n_s.at[e, k], n_r.at[e, k], f, s
        )

    def new_arrival(k, e):
        return remote(
            drecv.at[e, pl.ds(0, 128), :], dnew.at[(t + 8 - k) % 8, e],
            n_s.at[e, k], n_r.at[e, k], f, mate,
        )

    def back_copy(k, e):
        return remote(
            osend.at[e, at(to(k) * CAP, CAP, CAP), :], ret.at[e, f], b_s.at[e, k], b_r.at[e, k], to(k), t
        )

    def back_arrival(k, e):
        return remote(
            osend.at[e, pl.ds(0, CAP), :], ret.at[e, came(k)], b_s.at[e, k], b_r.at[e, k], f, mate
        )

    for e in range(2):
        for n, m in ((4, 7), (6, 8)):
            hidden_arrival(e, n).wait_recv()
            hidden_copy(e, m).start()
        for k in ORDER:
            down_arrival(k, e).wait_recv()
        for n in (2, 3, 5, 7, 8):
            hidden_arrival(e, n).wait_recv()

        def expert_out(g, carry):
            part = at(g * 192, 192, 192)
            h = jnp.concatenate([hid[s, e, part, :] for s in range(8)], axis=1)
            osend[e, part, :] = jnp.dot(h, drecv[e], preferred_element_type=F32).astype(BF)
            return carry

        lax.fori_loop(0, 4, expert_out, 0)
        for k in ORDER:
            back_copy(k, e).start()
        ret[e, f] = osend[e, at(f * CAP, CAP, CAP), :]
        for k in range(1, 8):
            new_copy(k, e).start()
        dnew[t, e] = drecv[e, at(t * 128, 128, 128), :]

    def new_out(s):
        return local(dnew.at[s], down_o.at[:, :, pl.ds(s * 512, 512)], o_s.at[2 + s])

    def mix(e):
        back = ret[e].reshape(768, 512)
        w_t = cols[...].T
        first = jnp.dot(comb[0, e], back, preferred_element_type=F32) * w_t[:, 2:3]
        second = jnp.dot(comb[1, e], back, preferred_element_type=F32) * w_t[:, 3:4]
        return first + second

    for k in ORDER:
        back_arrival(k, 0).wait_recv()
    macc[...] = mix(0)
    for e in range(2):
        for k in range(1, 8):
            new_arrival(k, e).wait_recv()
    for s in range(8):
        new_out(s).start()
    for k in ORDER:
        back_arrival(k, 1).wait_recv()
    mixed_o[...] = (macc[...] + mix(1)).astype(BF)

    for k in ORDER:
        token_copy(k).wait_send()
        for e in range(2):
            weights_pair(k, e).wait_send()
            down_copy(k, e).wait_send()
            back_copy(k, e).wait_send()
    for k in chain:
        for n in range(9):
            row_copy(k, n).wait_send()
    for e in range(2):
        for n in range(9):
            hidden_copy(e, n).wait_send()
        for k in range(1, 8):
            new_copy(k, e).wait_send()
    gate_out.wait()
    up_out.wait()
    for s in range(8):
        new_out(s).wait()


def on_device(
    prompt, expert_ids, group_weight, expert_share, norm_gain, gate_train, up_train, down_train
):
    any_ref = pl.BlockSpec(memory_space=pl.ANY)
    vmem_ref = pl.BlockSpec(memory_space=pltpu.VMEM)
    dma = pltpu.SemaphoreType.DMA
    return pl.pallas_call(
        kernel,
        out_shape=(
            jax.ShapeDtypeStruct((512, 512), BF),
            jax.ShapeDtypeStruct((2, 4096, 128), BF),
            jax.ShapeDtypeStruct((2, 4096, 128), BF),
            jax.ShapeDtypeStruct((2, 128, 4096), BF),
        ),
        in_specs=[any_ref, vmem_ref, vmem_ref, vmem_ref, vmem_ref, any_ref, any_ref, any_ref],
        out_specs=(vmem_ref, any_ref, any_ref, any_ref),
        scratch_shapes=[
            pltpu.VMEM((512, 4096), BF),
            pltpu.VMEM((512, 512), BF),
            pltpu.VMEM((512, 512), BF),
            pltpu.VMEM((256, 128), F32),
            pltpu.VMEM((16, 2, 256, 128), F32),
            pltpu.VMEM((16, 2, 256, 128), F32),
            pltpu.VMEM((8, 2, 64, 512), F32),
            pltpu.VMEM((16, 2, 2, 256, 128), BF),
            pltpu.VMEM((16, 2, 64, 512), BF),
            pltpu.VMEM((32, 512), F32),
            pltpu.VMEM((32, CAP, 512), BF),
            pltpu.VMEM((16, 2, CAP, 512), BF),
            pltpu.VMEM((8, 2, 768, 512), BF),
            pltpu.VMEM((2, 2, 4096, 128), BF),
            pltpu.VMEM((2, 1024, 512), BF),
            pltpu.VMEM((2, 768, 256), F32),
            pltpu.VMEM((8, 2, 768, 128), BF),
            pltpu.VMEM((2, 768, 512), BF),
            pltpu.VMEM((2, 16, CAP, 512), BF),
            pltpu.VMEM((128, 512), F32),
            pltpu.VMEM((2, 2, 512, 768), BF),
            pltpu.VMEM((512, 512), F32),
            pltpu.VMEM((8, 2, 128, 512), BF),
            dma((5,)), dma((16,)), dma((16,)), dma((8,)),
            dma((16,)), dma((16,)), dma((2, 16)), dma((2, 16)),
            dma((16, 9)), dma((16, 9)), dma((2, 9)), dma((2, 9)),
            dma((2, 16)), dma((2, 16)), dma((2, 8)), dma((2, 8)),
            dma((2, 16)), dma((2, 16)), dma((10,)),
        ],
        compiler_params=pltpu.CompilerParams(
            collective_id=0, has_side_effects=True, vmem_limit_bytes=67043328
        ),
        name="handover",
    )(
        prompt,
        expert_ids.T,
        group_weight.reshape(1, -1),
        expert_share.T,
        norm_gain.reshape(1, -1),
        gate_train.reshape(16, 2, 256, 128),
        up_train.reshape(16, 2, 256, 128),
        down_train.reshape(16, 2, 64, 512),
    )


def solution(mesh):
    placed = (
        P("fs", None),
        P("fs", None),
        P("fs"),
        P("fs", None),
        P("fs"),
        P(None, "fs", "tp"),
        P(None, "fs", "tp"),
        P(None, "fs", "tp"),
    )
    return jax.shard_map(
        on_device,
        mesh=mesh,
        in_specs=placed,
        out_specs=(P("fs", "tp"), P("fs", None, "tp"), P("fs", None, "tp"), P("fs", "tp", None)),
        check_vma=False,
    )
```

```python
import jax
import jax.numpy as jnp
from jax import lax
from jax.experimental import pallas as pl
from jax.experimental.pallas import tpu as pltpu
from jax.sharding import PartitionSpec as P

MESH = pl.DeviceIdType.MESH
BF = jnp.bfloat16
F32 = jnp.float32
EPS = 1e-06
CAP = 48
ORDER = (4, 12, 1, 3, 5, 15, 7, 13, 8, 2, 10, 6, 14, 9, 11)


def kernel(
    prompt, ids_h, gw_h, share_h, gain_h, gate, up, down,
    gate_o, up_o, down_o, ret1, comb1, macc, shares,
    ids, gw, share, gain, pf, xn, gb, sw, sd, wsend, dsend, cm, tsend, rows, drecv,
    hid, stage, ret0, cols,
    i_s, l_s, s_s, t_r, w_r, x_r, x_b, h_r, d_r, n_r, b_r,
):
    f = lax.axis_index("fs")
    t = lax.axis_index("tp")
    z, y = f // 4, f % 4
    x, c = t // 2, t % 2
    right = ((x + 1) % 4) * 2 + c
    left = ((x + 3) % 4) * 2 + c
    across = ((x + 2) % 4) * 2 + c
    mate = x * 2 + 1 - c
    flip = 1 - 2 * c

    def to(k):
        return ((z + k // 4) % 4) * 4 + (y + k % 4) % 4

    def came(k):
        return ((z + 4 - k // 4) % 4) * 4 + (y + 4 - k % 4) % 4

    def at(start, size, unit):
        return pl.ds(pl.multiple_of(start, unit), size)

    def local(src, dst, sem):
        return pltpu.make_async_copy(src, dst, sem)

    def remote(src, dst, ssem, rsem, fs, tp):
        return pltpu.make_async_remote_copy(
            src_ref=src, dst_ref=dst, send_sem=ssem, recv_sem=rsem,
            device_id=(fs, tp), device_id_type=MESH,
        )

    def arrived(ref, sem):
        remote(ref, ref, s_s.at[0], sem, f, mate).wait_recv()

    def sent(ref, sem):
        remote(ref, ref, sem, n_r.at[0], f, mate).wait_send()

    barrier = pltpu.get_barrier_semaphore()

    def greet_fs(k, carry):
        pl.semaphore_signal(barrier, inc=1, device_id=(to(k), t), device_id_type=MESH)
        return carry

    def greet_tp(k, carry):
        pl.semaphore_signal(barrier, inc=1, device_id=(f, (t + k) % 8), device_id_type=MESH)
        return carry

    lax.fori_loop(1, 16, greet_fs, 0)
    lax.fori_loop(1, 8, greet_tp, 0)

    chain = (0,) + ORDER
    source = (gate, up)
    fresh = (gate_o, up_o)
    ret = (ret0, ret1)
    comb = (pf, comb1)

    def load_weights(i, e, m, sem):
        return local(source[m].at[to(chain[(i + 1) % 16]), e], sw.at[i, m], l_s.at[sem])

    small = [
        local(src, dst, i_s.at[n])
        for n, (src, dst) in enumerate(((ids_h, ids), (gw_h, gw), (share_h, share), (gain_h, gain)))
    ]
    for load in small:
        load.start()
    for i in range(8):
        load_weights(i, 0, 0, 0).start()
    for i in range(16):
        local(prompt.at[:, i * 256 : (i + 1) * 256], pf.at[i], l_s.at[1]).start()
    for i in range(16):
        for m in range(2):
            if i > 7 or m:
                load_weights(i, 0, m, 2).start()

    for load in small:
        load.wait()
    gb[...] = jnp.broadcast_to(gain[...], (128, 256)).T

    def rank_slots():
        expert = lax.broadcasted_iota(jnp.int32, (32, 512), 0)
        hit0 = ids[0:1, :] == expert
        hit1 = ids[1:2, :] == expert
        named = jnp.where(hit0 | hit1, 1.0, 0.0)
        before = jnp.where(
            lax.broadcasted_iota(jnp.int32, (512, 512), 0)
            < lax.broadcasted_iota(jnp.int32, (512, 512), 1), 1.0, 0.0,
        ).astype(BF)
        count = jnp.dot(named.astype(BF), before, preferred_element_type=F32)
        cm[...] = jnp.where(named > 0.5, count, -1.0)
        total = share[0:1, :] + share[1:2, :]
        for k, hit in ((0, hit0), (1, hit1)):
            rank = jnp.sum(jnp.where(hit, count, 0.0), axis=0, keepdims=True)
            expert_of = ids[k : k + 1, :]
            place = (expert_of & 1) * 768 + (expert_of >> 1) * CAP
            cols[k : k + 1, :] = place.astype(F32) + rank
            cols[k + 2 : k + 3, :] = gw[...] * share[k : k + 1, :] / total

    cols[...] = jnp.zeros_like(cols)
    rank_slots()

    def build_pick(e, carry):
        slot = lax.broadcasted_iota(jnp.int32, (CAP, 512), 0).astype(F32)
        stage[e] = jnp.where(cm[pl.ds(e, 1), :] == slot, 1.0, 0.0).astype(BF)
        return carry

    lax.fori_loop(0, 32, build_pick, 0)

    def cast_weights(i, e, m):
        wsend[chain[(i + 1) % 16], e, m] = (sw[i, m] * gb[...]).astype(BF)

    def weights_copy(k, e, m):
        return remote(
            wsend.at[k, e, m], fresh[m].at[e, at(f * 256, 256, 256), :],
            s_s.at[0], w_r.at[e, m], to(k), t,
        )

    local(sw.at[pl.ds(0, 8), 0], sw.at[pl.ds(0, 8), 0], l_s.at[0]).wait()
    for i in range(8):
        cast_weights(i, 0, 0)
    pl.semaphore_wait(barrier, 22)
    for k in ORDER[:8]:
        weights_copy(k, 0, 0).start()

    local(pf, pf, l_s.at[1]).wait()

    def normalize(i, carry):
        block = at(i * 32, 32, 32)
        squares = jnp.zeros((32, 256), F32)
        for j in range(16):
            part = pf[j, block, :].astype(F32)
            squares = squares + part * part
        mean = jnp.sum(squares, axis=1, keepdims=True) * (1.0 / 4096.0)
        scale = lax.rsqrt(mean + EPS)
        for h in range(2):
            part = pf[2 * t + h, block, :].astype(F32)
            xn[block, h * 256 : (h + 1) * 256] = (part * scale).astype(BF)
        return carry

    lax.fori_loop(0, 16, normalize, 0, unroll=4)

    for g in range(4):
        chosen = stage[g * 8 : g * 8 + 8].reshape(384, 512)
        tsend[4 * g : 4 * g + 4] = (
            jnp.dot(chosen, xn[...], preferred_element_type=F32).astype(BF).reshape(4, 2, CAP, 512)
        )

    def token_copy(k):
        return remote(
            tsend.at[to(k)], rows.at[t, :, at(f * CAP, CAP, CAP), :],
            s_s.at[1], t_r.at[k], to(k), t,
        )

    for k in ORDER:
        token_copy(k).start()
    rows[t, :, at(f * CAP, CAP, CAP), :] = tsend[f]

    local(sw.at[pl.ds(0, 12)], sw.at[pl.ds(0, 12)], l_s.at[2]).wait()
    for m in range(2):
        for i in range(16):
            if i > 7 or m:
                cast_weights(i, 0, m)
    for k in ORDER[8:]:
        weights_copy(k, 0, 0).start()
    for k in ORDER:
        weights_copy(k, 0, 1).start()
    for i in range(16):
        for m in range(2):
            load_weights(i, 1, m, 3).start()

    def load_down(i):
        return local(down.at[to(chain[i])], sd.at[pl.ds(i % 8 * 2, 2)], l_s.at[4])

    for i in range(8):
        load_down(i).start()

    def row_copy(k, n):
        r = at(came(k) * CAP, CAP, CAP)
        both = {0: (t, right), 1: (t, left), 2: (t, mate), 3: (left, mate), 5: (right, mate)}
        if n in both:
            s, who = both[n]
            ref = rows.at[s, :, r, :]
        else:
            s, e, who = {4: (left, 0, right), 6: (right, 1, left), 7: (across, 0, mate), 8: (across, 1, mate)}[n]
            ref = rows.at[s, e, r, :]
        slot = {0: 0, 1: 1, 4: 2, 6: 3}
        i = chain.index(k) // 2
        sem = x_r.at[i, slot[n]] if n in slot else x_b.at[n // 7]
        return remote(ref, ref, s_s.at[2], sem, f, who)

    pair = pl.ds(0, 2 * CAP)

    def token_round(part):
        for k in part:
            if k:
                arrived(tsend.at[0], t_r.at[k])
            for n in range(3):
                row_copy(k, n).start()

    token_round(chain[:6])
    local(sw, sw, l_s.at[3]).wait()
    for m in range(2):
        for i in range(16):
            cast_weights(i, 1, m)
        for k in ORDER:
            weights_copy(k, 1, m).start()
    for m in range(2):
        fresh[m][:, at(f * 256, 256, 256), :] = wsend[0, :, m]
    token_round(chain[6:])

    def down_copy(k, e):
        return remote(
            dsend.at[k, e], drecv.at[e, at(f * 64, 64, 64), :], s_s.at[3], d_r.at[e], to(k), t
        )

    def cast_down(base):
        local(sd, sd, l_s.at[4]).wait()
        for i in range(8):
            for e in range(2):
                dsend[chain[base + i], e] = sd[2 * i + e].astype(BF)

    def relay(i):
        arrived(rows.at[left, :, pair, :], x_r.at[i, 0])
        for k in chain[2 * i : 2 * i + 2]:
            row_copy(k, 4).start()
            row_copy(k, 3).start()
        arrived(rows.at[right, :, pair, :], x_r.at[i, 1])
        for k in chain[2 * i : 2 * i + 2]:
            row_copy(k, 6).start()
            row_copy(k, 5).start()

    cast_down(0)
    for i in range(8, 16):
        load_down(i).start()
    for i in range(3):
        relay(i)
    cast_down(8)
    drecv[:, at(f * 64, 64, 64), :] = dsend[0]
    for e in range(2):
        for k in ORDER:
            down_copy(k, e).start()
    for i in range(3, 6):
        relay(i)
    cols_t = cols[...].T
    lane = lax.broadcasted_iota(jnp.int32, (512, 256), 1).astype(F32)
    for k in range(2):
        for n in range(6):
            hit = cols_t[:, k : k + 1] == lane + 256.0 * n
            comb[n // 3][k * 3 + n % 3] = jnp.where(hit, 1.0, 0.0).astype(BF)
    shares[...] = cols_t
    for i in range(6, 8):
        relay(i)

    def project(e, chip):
        part = at(chip * 1024, 1024, 1024)
        left_side = jnp.concatenate([rows[2 * chip, e], rows[2 * chip + 1, e]], axis=1)
        both = jnp.concatenate([gate_o[e, part, :], up_o[e, part, :]], axis=1)
        return jnp.dot(left_side, both, preferred_element_type=F32)

    def total(e):
        return sd.at[pl.ds(0, 12), :, pl.ds(e * 256, 256)]

    def near(e):
        total(e)[...] = project(e, x).reshape(12, 64, 256)

        def step(j, carry):
            total(e)[...] += project(e, (x + j + j // 2) % 4).reshape(12, 64, 256)
            return carry

        lax.fori_loop(1, 3, step, 0)

    def finish(e):
        last = project(e, (x + 2) % 4) + total(e)[...].reshape(768, 256)
        v = last[:, 0:128]
        hid[t, e] = (v / (1.0 + jnp.exp(-v)) * last[:, 128:256]).astype(BF)

    def hidden_ref(s, e, part):
        return hid.at[s, e] if part is None else hid.at[s, e, pl.ds(part * 384, 384), :]

    def hidden_copy(e, n):
        s, part, who = (
            (t, None, right), (t, None, left), (t, None, mate), (left, None, mate), (left, 0, right),
            (right, None, mate), (right, 1, left), (across, 0, mate), (across, 1, mate),
        )[n]
        ref = hidden_ref(s, e, part)
        slot = {0: 0, 1: 1, 4: 2, 6: 3}.get(n, 4)
        return remote(ref, ref, s_s.at[4], h_r.at[e, slot], f, who)

    half = pl.ds(0, 384)

    for m in range(2):
        arrived(fresh[m].at[0, pl.ds(0, 3840), :], w_r.at[0, m])
    arrived(rows.at[pl.ds(0, 3)], x_b.at[0])
    near(0)
    for i in range(8):
        arrived(rows.at[across, 0, pair, :], x_r.at[i, 2])
        for k in chain[2 * i : 2 * i + 2]:
            row_copy(k, 7).start()
        arrived(rows.at[across, 1, pair, :], x_r.at[i, 3])
        for k in chain[2 * i : 2 * i + 2]:
            row_copy(k, 8).start()
    arrived(rows.at[0], x_b.at[1])
    finish(0)
    for n in range(3):
        hidden_copy(0, n).start()
    for m in range(2):
        arrived(fresh[m].at[1, pl.ds(0, 3840), :], w_r.at[1, m])
    near(1)
    finish(1)
    for n in range(3):
        hidden_copy(1, n).start()

    for e in range(2):
        arrived(hid.at[left, e], h_r.at[e, 0])
        hidden_copy(e, 4).start()
        hidden_copy(e, 3).start()
        arrived(hid.at[right, e], h_r.at[e, 1])
        hidden_copy(e, 6).start()
        hidden_copy(e, 5).start()

    def new_copy(k, e):
        s = (t + k) % 8
        return remote(
            drecv.at[e, at(s * 128, 128, 128), :], down_o.at[e, :, at(t * 512, 512, 512)],
            s_s.at[5], n_r.at[0], f, s,
        )

    def back_copy(k, e):
        return remote(
            stage.at[e * 16 + to(k)], ret[e].at[f], s_s.at[6], b_r.at[e], to(k), t
        )

    for e in range(2):
        for n in range(2):
            arrived(hid.at[across, e, half, :], h_r.at[e, 2 + n])
            hidden_copy(e, 7 + n).start()
        arrived(drecv.at[e, pl.ds(0, 960), :], d_r.at[e])
        arrived(hid.at[pl.ds(0, 4), e], h_r.at[e, 4])

        def expert_out(g, carry):
            part = at(g * 192, 192, 192)
            h = jnp.concatenate([hid[s, e, part, :] for s in range(8)], axis=1)
            out = jnp.dot(h, drecv[e], preferred_element_type=F32).astype(BF)
            stage[pl.ds(e * 16 + g * 4, 4)] = out.reshape(4, CAP, 512)
            return carry

        lax.fori_loop(0, 4, expert_out, 0)
        for k in ORDER:
            back_copy(k, e).start()
        ret[e][f] = stage[e * 16 + f]
        for k in range(1, 8):
            new_copy(k, e).start()
        down_o[e, :, at(t * 512, 512, 512)] = drecv[e, at(t * 128, 128, 128), :]

    arrived(ret0.at[pl.ds(0, 15)], b_r.at[0])
    macc[...] = mix(pf, ret0, shares, pl.ds(0, 512))
    arrived(down_o.at[:, :, pl.ds(0, 3584)], n_r.at[0])
    arrived(ret1.at[pl.ds(0, 15)], b_r.at[1])
    sent(wsend.at[pl.ds(0, 15)], s_s.at[0])
    sent(tsend.at[pl.ds(0, 15)], s_s.at[1])
    sent(rows.at[pl.ds(0, 7)], s_s.at[2])
    sent(dsend.at[pl.ds(0, 15)], s_s.at[3])
    sent(hid.at[pl.ds(0, 7)], s_s.at[4])
    sent(down_o.at[:, :, pl.ds(0, 3584)], s_s.at[5])
    sent(stage.at[pl.ds(0, 30)], s_s.at[6])


def mix(comb, ret, shares, part):
    total = 0.0
    for k in range(2):
        picked = 0.0
        for n in range(3):
            back = ret[...].reshape(768, 512)[n * 256 : (n + 1) * 256]
            picked += jnp.dot(comb[k * 3 + n, part, :], back, preferred_element_type=F32)
        total += picked * shares[part, 2 + k : 3 + k]
    return total


def settle(gate, up, down, ret1, comb1, macc, shares, mixed_o, gate_o, up_o, down_o, mixed, sem):
    moves = [
        pltpu.make_async_copy(src, dst, sem.at[n])
        for n, (src, dst) in enumerate(((gate, gate_o), (up, up_o), (down, down_o)))
    ]
    for move in moves:
        move.start()
    for n in range(4):
        part = pl.ds(n * 128, 128)
        mixed[part, :] = (macc[part, :] + mix(comb1, ret1, shares, part)).astype(BF)
        moves.append(pltpu.make_async_copy(mixed.at[part], mixed_o.at[part], sem.at[3 + n]))
        moves[-1].start()
    for move in moves:
        move.wait()


def on_device(
    prompt, expert_ids, group_weight, expert_share, norm_gain, gate_train, up_train, down_train
):
    any_ref = pl.BlockSpec(memory_space=pl.ANY)
    vmem_ref = pl.BlockSpec(memory_space=pltpu.VMEM)
    hbm_ref = pl.BlockSpec(memory_space=pltpu.HBM)
    dma = pltpu.SemaphoreType.DMA
    made = pl.pallas_call(
        kernel,
        out_shape=(
            jax.ShapeDtypeStruct((2, 4096, 128), BF),
            jax.ShapeDtypeStruct((2, 4096, 128), BF),
            jax.ShapeDtypeStruct((2, 128, 4096), BF),
            jax.ShapeDtypeStruct((16, CAP, 512), BF),
            jax.ShapeDtypeStruct((6, 512, 256), BF),
            jax.ShapeDtypeStruct((512, 512), F32),
            jax.ShapeDtypeStruct((512, 128), F32),
        ),
        in_specs=[hbm_ref] * 8,
        out_specs=(vmem_ref,) * 7,
        scratch_shapes=[
            pltpu.VMEM((2, 512), jnp.int32),
            pltpu.VMEM((1, 512), F32),
            pltpu.VMEM((2, 512), F32),
            pltpu.VMEM((1, 256), F32),
            pltpu.VMEM((16, 512, 256), BF),
            pltpu.VMEM((512, 512), BF),
            pltpu.VMEM((256, 128), F32),
            pltpu.VMEM((16, 2, 256, 128), F32),
            pltpu.VMEM((16, 64, 512), F32),
            pltpu.VMEM((16, 2, 2, 256, 128), BF),
            pltpu.VMEM((16, 2, 64, 512), BF),
            pltpu.VMEM((32, 512), F32),
            pltpu.VMEM((16, 2, CAP, 512), BF),
            pltpu.VMEM((8, 2, 768, 512), BF),
            pltpu.VMEM((2, 1024, 512), BF),
            pltpu.VMEM((8, 2, 768, 128), BF),
            pltpu.VMEM((32, CAP, 512), BF),
            pltpu.VMEM((16, CAP, 512), BF),
            pltpu.VMEM((128, 512), F32),
            dma((4,)), dma((5,)), dma((7,)), dma((16,)), dma((2, 2)), dma((8, 4)), dma((2,)),
            dma((2, 5)), dma((2,)), dma((1,)), dma((2,)),
        ],
        compiler_params=pltpu.CompilerParams(
            collective_id=0, has_side_effects=True, vmem_limit_bytes=45500000
        ),
        name="handover",
    )(
        prompt,
        expert_ids.T,
        group_weight.reshape(1, -1),
        expert_share.T,
        norm_gain.reshape(1, -1),
        gate_train.reshape(16, 2, 256, 128),
        up_train.reshape(16, 2, 256, 128),
        down_train.reshape(16, 2, 64, 512),
    )

    return pl.pallas_call(
        settle,
        out_shape=(
            jax.ShapeDtypeStruct((512, 512), BF),
            jax.ShapeDtypeStruct((2, 4096, 128), BF),
            jax.ShapeDtypeStruct((2, 4096, 128), BF),
            jax.ShapeDtypeStruct((2, 128, 4096), BF),
        ),
        in_specs=[any_ref] * 3 + [vmem_ref] * 4,
        out_specs=(hbm_ref,) * 4,
        scratch_shapes=[pltpu.VMEM((512, 512), BF), dma((7,))],
        compiler_params=pltpu.CompilerParams(vmem_limit_bytes=6 << 20),
        name="settle",
    )(*made)


def solution(mesh):
    placed = (
        P("fs", None),
        P("fs", None),
        P("fs"),
        P("fs", None),
        P("fs"),
        P(None, "fs", "tp"),
        P(None, "fs", "tp"),
        P(None, "fs", "tp"),
    )
    return jax.shard_map(
        on_device,
        mesh=mesh,
        in_specs=placed,
        out_specs=(P("fs", "tp"), P("fs", None, "tp"), P("fs", None, "tp"), P("fs", "tp", None)),
        check_vma=False,
    )
```

```python
import jax
import jax.numpy as jnp
from jax import lax
from jax.experimental import pallas as pl
from jax.experimental.pallas import tpu as pltpu
from jax.sharding import PartitionSpec as P

MESH = pl.DeviceIdType.MESH
BF = jnp.bfloat16
F32 = jnp.float32
EPS = 1e-06
CAP = 48
ORDER = (4, 12, 1, 3, 5, 15, 7, 13, 8, 2, 10, 6, 14, 9, 11)


def kernel(
    prompt, ids, gain, gate, up, down,
    gate_o, up_o, down_o, ret1, comb1, picked0,
    pf, xn, gb, sw, sd, wsend, dsend, cm, tsend, rows, drecv,
    hid, stage, ret0, cols,
    l_s, s_s, t_r, w_r, x_r, x_b, h_r, d_r, n_r, b_r,
):
    f = lax.axis_index("fs")
    t = lax.axis_index("tp")
    z, y = f // 4, f % 4
    x, c = t // 2, t % 2
    right = ((x + 1) % 4) * 2 + c
    left = ((x + 3) % 4) * 2 + c
    across = ((x + 2) % 4) * 2 + c
    mate = x * 2 + 1 - c
    flip = 1 - 2 * c

    def to(k):
        return ((z + k // 4) % 4) * 4 + (y + k % 4) % 4

    def came(k):
        return ((z + 4 - k // 4) % 4) * 4 + (y + 4 - k % 4) % 4

    def at(start, size, unit):
        return pl.ds(pl.multiple_of(start, unit), size)

    def local(src, dst, sem):
        return pltpu.make_async_copy(src, dst, sem)

    def remote(src, dst, ssem, rsem, fs, tp):
        return pltpu.make_async_remote_copy(
            src_ref=src, dst_ref=dst, send_sem=ssem, recv_sem=rsem,
            device_id=(fs, tp), device_id_type=MESH,
        )

    def arrived(ref, sem):
        remote(ref, ref, s_s.at[0], sem, f, mate).wait_recv()

    def sent(ref, sem):
        remote(ref, ref, sem, n_r.at[0], f, mate).wait_send()

    barrier = pltpu.get_barrier_semaphore()

    def greet_fs(k, carry):
        pl.semaphore_signal(barrier, inc=1, device_id=(to(k), t), device_id_type=MESH)
        return carry

    def greet_tp(k, carry):
        pl.semaphore_signal(barrier, inc=1, device_id=(f, (t + k) % 8), device_id_type=MESH)
        return carry

    lax.fori_loop(1, 16, greet_fs, 0)
    lax.fori_loop(1, 8, greet_tp, 0)

    chain = (0,) + ORDER
    source = (gate, up)
    fresh = (gate_o, up_o)
    ret = (ret0, ret1)
    comb = (pf, comb1)

    def load_weights(i, e, m, sem):
        return local(source[m].at[to(chain[(i + 1) % 16]), e], sw.at[i, m], l_s.at[sem])

    for i in range(16):
        local(prompt.at[:, i * 256 : (i + 1) * 256], pf.at[i], l_s.at[1]).start()
    for i in range(8):
        load_weights(i, 0, 0, 0).start()
    for i in range(16):
        for m in range(2):
            if i > 7 or m:
                load_weights(i, 0, m, 2).start()

    gb[...] = jnp.broadcast_to(gain[...], (128, 256)).T

    def rank_slots():
        expert = lax.broadcasted_iota(jnp.int32, (32, 512), 0).astype(F32)
        hit0 = ids[0:1, :] == expert
        hit1 = ids[1:2, :] == expert
        named = jnp.where(hit0 | hit1, 1.0, 0.0)
        before = jnp.where(
            lax.broadcasted_iota(jnp.int32, (512, 512), 0)
            < lax.broadcasted_iota(jnp.int32, (512, 512), 1), 1.0, 0.0,
        ).astype(BF)
        count = jnp.dot(named.astype(BF), before, preferred_element_type=F32)
        cm[...] = jnp.where(named > 0.5, count, -1.0)
        for k, hit in ((0, hit0), (1, hit1)):
            rank = jnp.sum(jnp.where(hit, count, 0.0), axis=0, keepdims=True)
            expert_of = ids[k : k + 1, :]
            pair = jnp.floor(expert_of * 0.5)
            place = (expert_of - 2.0 * pair) * 768.0 + pair * float(CAP)
            cols[k : k + 1, :] = place + rank

    cols[...] = jnp.zeros_like(cols)
    rank_slots()

    def build_pick(e, carry):
        slot = lax.broadcasted_iota(jnp.int32, (CAP, 512), 0).astype(F32)
        stage[e] = jnp.where(cm[pl.ds(e, 1), :] == slot, 1.0, 0.0).astype(BF)
        return carry

    lax.fori_loop(0, 32, build_pick, 0)

    def cast_weights(i, e, m):
        wsend[chain[(i + 1) % 16], e, m] = (sw[i, m] * gb[...]).astype(BF)

    def weights_copy(k, e, m):
        return remote(
            wsend.at[k, e, m], fresh[m].at[e, at(f * 256, 256, 256), :],
            s_s.at[0], w_r.at[e, m], to(k), t,
        )

    local(pf, pf, l_s.at[1]).wait()

    def normalize(i, carry):
        block = at(i * 32, 32, 32)
        squares = jnp.zeros((32, 256), F32)
        for j in range(16):
            part = pf[j, block, :].astype(F32)
            squares = squares + part * part
        mean = jnp.sum(squares, axis=1, keepdims=True) * (1.0 / 4096.0)
        scale = lax.rsqrt(mean + EPS)
        for h in range(2):
            part = pf[2 * t + h, block, :].astype(F32)
            xn[block, h * 256 : (h + 1) * 256] = (part * scale).astype(BF)
        return carry

    lax.fori_loop(0, 16, normalize, 0, unroll=4)

    for g in range(4):
        chosen = stage[g * 8 : g * 8 + 8].reshape(384, 512)
        tsend[4 * g : 4 * g + 4] = (
            jnp.dot(chosen, xn[...], preferred_element_type=F32).astype(BF).reshape(4, 2, CAP, 512)
        )

    def token_copy(k):
        return remote(
            tsend.at[to(k)], rows.at[t, :, at(f * CAP, CAP, CAP), :],
            s_s.at[1], t_r.at[k], to(k), t,
        )

    pl.semaphore_wait(barrier, 22)
    for k in ORDER:
        token_copy(k).start()
    rows[t, :, at(f * CAP, CAP, CAP), :] = tsend[f]

    local(sw.at[pl.ds(0, 8), 0], sw.at[pl.ds(0, 8), 0], l_s.at[0]).wait()
    for i in range(8):
        cast_weights(i, 0, 0)
    for k in ORDER[:8]:
        weights_copy(k, 0, 0).start()
    local(sw.at[pl.ds(0, 12)], sw.at[pl.ds(0, 12)], l_s.at[2]).wait()
    for m in range(2):
        for i in range(16):
            if i > 7 or m:
                cast_weights(i, 0, m)
    for k in ORDER[8:]:
        weights_copy(k, 0, 0).start()
    for k in ORDER:
        weights_copy(k, 0, 1).start()
    for i in range(16):
        for m in range(2):
            load_weights(i, 1, m, 3).start()

    def load_down(i):
        return local(down.at[to(chain[i])], sd.at[pl.ds(i % 8 * 2, 2)], l_s.at[4])

    for i in range(8):
        load_down(i).start()

    def row_copy(k, n):
        r = at(came(k) * CAP, CAP, CAP)
        both = {0: (t, right), 1: (t, left), 2: (t, mate), 3: (left, mate), 5: (right, mate)}
        if n in both:
            s, who = both[n]
            ref = rows.at[s, :, r, :]
        else:
            s, e, who = {4: (left, 0, right), 6: (right, 1, left), 7: (across, 0, mate), 8: (across, 1, mate)}[n]
            ref = rows.at[s, e, r, :]
        slot = {0: 0, 1: 1, 4: 2, 6: 3}
        i = chain.index(k) // 2
        sem = x_r.at[i, slot[n]] if n in slot else x_b.at[n // 7]
        return remote(ref, ref, s_s.at[2], sem, f, who)

    pair = pl.ds(0, 2 * CAP)

    def token_round(part):
        for k in part:
            if k:
                arrived(tsend.at[0], t_r.at[k])
            for n in range(3):
                row_copy(k, n).start()

    token_round(chain[:6])
    local(sw, sw, l_s.at[3]).wait()
    for m in range(2):
        for i in range(16):
            cast_weights(i, 1, m)
        for k in ORDER:
            weights_copy(k, 1, m).start()
    for m in range(2):
        fresh[m][:, at(f * 256, 256, 256), :] = wsend[0, :, m]
    token_round(chain[6:])

    def down_copy(k, e):
        return remote(
            dsend.at[k, e], drecv.at[e, at(f * 64, 64, 64), :], s_s.at[3], d_r.at[e], to(k), t
        )

    def cast_down(base):
        local(sd, sd, l_s.at[4]).wait()
        for i in range(8):
            for e in range(2):
                dsend[chain[base + i], e] = sd[2 * i + e].astype(BF)

    def relay(i):
        arrived(rows.at[left, :, pair, :], x_r.at[i, 0])
        for k in chain[2 * i : 2 * i + 2]:
            row_copy(k, 4).start()
            row_copy(k, 3).start()
        arrived(rows.at[right, :, pair, :], x_r.at[i, 1])
        for k in chain[2 * i : 2 * i + 2]:
            row_copy(k, 6).start()
            row_copy(k, 5).start()

    cast_down(0)
    for i in range(8, 16):
        load_down(i).start()
    for i in range(3):
        relay(i)
    cast_down(8)
    drecv[:, at(f * 64, 64, 64), :] = dsend[0]
    for e in range(2):
        for k in ORDER:
            down_copy(k, e).start()
    for i in range(3, 6):
        relay(i)
    cols_t = cols[...].T
    lane = lax.broadcasted_iota(jnp.int32, (512, 256), 1).astype(F32)
    for k in range(2):
        for n in range(6):
            hit = cols_t[:, k : k + 1] == lane + 256.0 * n
            comb[n // 3][k * 3 + n % 3] = jnp.where(hit, 1.0, 0.0).astype(BF)
    for i in range(6, 8):
        relay(i)

    def project(e, chip):
        part = at(chip * 1024, 1024, 1024)
        left_side = jnp.concatenate([rows[2 * chip, e], rows[2 * chip + 1, e]], axis=1)
        both = jnp.concatenate([gate_o[e, part, :], up_o[e, part, :]], axis=1)
        return jnp.dot(left_side, both, preferred_element_type=F32)

    def total(e):
        return sd.at[pl.ds(0, 12), :, pl.ds(e * 256, 256)]

    def near(e):
        total(e)[...] = project(e, x).reshape(12, 64, 256)

        def step(j, carry):
            total(e)[...] += project(e, (x + j + j // 2) % 4).reshape(12, 64, 256)
            return carry

        lax.fori_loop(1, 3, step, 0)

    def finish(e):
        last = project(e, (x + 2) % 4) + total(e)[...].reshape(768, 256)
        v = last[:, 0:128]
        hid[t, e] = (v / (1.0 + jnp.exp(-v)) * last[:, 128:256]).astype(BF)

    def hidden_ref(s, e, part):
        return hid.at[s, e] if part is None else hid.at[s, e, pl.ds(part * 384, 384), :]

    def hidden_copy(e, n):
        s, part, who = (
            (t, None, right), (t, None, left), (t, None, mate), (left, None, mate), (left, 0, right),
            (right, None, mate), (right, 1, left), (across, 0, mate), (across, 1, mate),
        )[n]
        ref = hidden_ref(s, e, part)
        slot = {0: 0, 1: 1, 4: 2, 6: 3}.get(n, 4)
        return remote(ref, ref, s_s.at[4], h_r.at[e, slot], f, who)

    half = pl.ds(0, 384)

    for m in range(2):
        arrived(fresh[m].at[0, pl.ds(0, 3840), :], w_r.at[0, m])
    arrived(rows.at[pl.ds(0, 3)], x_b.at[0])
    near(0)
    for i in range(8):
        arrived(rows.at[across, 0, pair, :], x_r.at[i, 2])
        for k in chain[2 * i : 2 * i + 2]:
            row_copy(k, 7).start()
        arrived(rows.at[across, 1, pair, :], x_r.at[i, 3])
        for k in chain[2 * i : 2 * i + 2]:
            row_copy(k, 8).start()
    arrived(rows.at[0], x_b.at[1])
    finish(0)
    for n in range(3):
        hidden_copy(0, n).start()
    for m in range(2):
        arrived(fresh[m].at[1, pl.ds(0, 3840), :], w_r.at[1, m])
    near(1)
    finish(1)
    for n in range(3):
        hidden_copy(1, n).start()

    for e in range(2):
        arrived(hid.at[left, e], h_r.at[e, 0])
        hidden_copy(e, 4).start()
        hidden_copy(e, 3).start()
        arrived(hid.at[right, e], h_r.at[e, 1])
        hidden_copy(e, 6).start()
        hidden_copy(e, 5).start()

    def new_copy(k, e):
        s = (x + k // 2) % 4 * 2 + (c + k) % 2
        return remote(
            drecv.at[e, at(s * 128, 128, 128), :], down_o.at[e, :, at(t * 512, 512, 512)],
            s_s.at[5], n_r.at[0], f, s,
        )

    def back_copy(k, e):
        return remote(
            stage.at[e * 16 + to(k)], ret[e].at[f], s_s.at[6], b_r.at[e], to(k), t
        )

    for e in range(2):
        for n in range(2):
            arrived(hid.at[across, e, half, :], h_r.at[e, 2 + n])
            hidden_copy(e, 7 + n).start()
        arrived(drecv.at[e, pl.ds(0, 960), :], d_r.at[e])
        for k in (2, 6, 3, 7, 4, 5, 1):
            new_copy(k, e).start()
        arrived(hid.at[pl.ds(0, 4), e], h_r.at[e, 4])

        def expert_out(g, carry):
            part = at(g * 192, 192, 192)
            h = jnp.concatenate([hid[s, e, part, :] for s in range(8)], axis=1)
            out = jnp.dot(h, drecv[e], preferred_element_type=F32).astype(BF)
            stage[pl.ds(e * 16 + g * 4, 4)] = out.reshape(4, CAP, 512)
            return carry

        lax.fori_loop(0, 4, expert_out, 0)
        for k in ORDER:
            back_copy(k, e).start()
        ret[e][f] = stage[e * 16 + f]
        down_o[e, :, at(t * 512, 512, 512)] = drecv[e, at(t * 128, 128, 128), :]

    arrived(ret0.at[pl.ds(0, 15)], b_r.at[0])
    for k in range(2):
        picked0[k] = pick_rows(pf, ret0, k, pl.ds(0, 512)).astype(BF)
    arrived(down_o.at[:, :, pl.ds(0, 3584)], n_r.at[0])
    arrived(ret1.at[pl.ds(0, 15)], b_r.at[1])
    sent(wsend.at[pl.ds(0, 15)], s_s.at[0])
    sent(tsend.at[pl.ds(0, 15)], s_s.at[1])
    sent(rows.at[pl.ds(0, 7)], s_s.at[2])
    sent(dsend.at[pl.ds(0, 15)], s_s.at[3])
    sent(hid.at[pl.ds(0, 7)], s_s.at[4])
    sent(down_o.at[:, :, pl.ds(0, 3584)], s_s.at[5])
    sent(stage.at[pl.ds(0, 30)], s_s.at[6])


def pick_rows(comb, ret, k, part):
    picked = 0.0
    for n in range(3):
        back = ret[...].reshape(768, 512)[n * 256 : (n + 1) * 256]
        picked += jnp.dot(comb[k * 3 + n, part, :], back, preferred_element_type=F32)
    return picked


def settle(
    gate, up, down, ret1, comb1, picked0, gw, share,
    mixed_o, gate_o, up_o, down_o, mixed, weight, sem,
):
    moves = [
        pltpu.make_async_copy(src, dst, sem.at[n])
        for n, (src, dst) in enumerate(((gate, gate_o), (up, up_o), (down, down_o)))
    ]
    for move in moves:
        move.start()
    total = share[0:1, :] + share[1:2, :]
    for k in range(2):
        row = gw[...] * share[k : k + 1, :] / total
        weight[k] = jnp.broadcast_to(row, (128, 512)).T
    for n in range(4):
        part = pl.ds(n * 128, 128)
        sums = []
        for k in range(2):
            value = picked0[k, part, :].astype(F32) + pick_rows(comb1, ret1, k, part)
            sums.append(value * weight[k, part, 0:1])
        mixed[part, :] = (sums[0] + sums[1]).astype(BF)
        moves.append(pltpu.make_async_copy(mixed.at[part], mixed_o.at[part], sem.at[3 + n]))
        moves[-1].start()
    for move in moves:
        move.wait()


def on_device(
    prompt, expert_ids, group_weight, expert_share, norm_gain, gate_train, up_train, down_train
):
    any_ref = pl.BlockSpec(memory_space=pl.ANY)
    vmem_ref = pl.BlockSpec(memory_space=pltpu.VMEM)
    hbm_ref = pl.BlockSpec(memory_space=pltpu.HBM)
    dma = pltpu.SemaphoreType.DMA
    made = pl.pallas_call(
        kernel,
        out_shape=(
            jax.ShapeDtypeStruct((2, 4096, 128), BF),
            jax.ShapeDtypeStruct((2, 4096, 128), BF),
            jax.ShapeDtypeStruct((2, 128, 4096), BF),
            jax.ShapeDtypeStruct((16, CAP, 512), BF),
            jax.ShapeDtypeStruct((6, 512, 256), BF),
            jax.ShapeDtypeStruct((2, 512, 512), BF),
        ),
        in_specs=[hbm_ref, vmem_ref, vmem_ref] + [hbm_ref] * 3,
        out_specs=(vmem_ref,) * 6,
        scratch_shapes=[
            pltpu.VMEM((16, 512, 256), BF),
            pltpu.VMEM((512, 512), BF),
            pltpu.VMEM((256, 128), F32),
            pltpu.VMEM((16, 2, 256, 128), F32),
            pltpu.VMEM((16, 64, 512), F32),
            pltpu.VMEM((16, 2, 2, 256, 128), BF),
            pltpu.VMEM((16, 2, 64, 512), BF),
            pltpu.VMEM((32, 512), F32),
            pltpu.VMEM((16, 2, CAP, 512), BF),
            pltpu.VMEM((8, 2, 768, 512), BF),
            pltpu.VMEM((2, 1024, 512), BF),
            pltpu.VMEM((8, 2, 768, 128), BF),
            pltpu.VMEM((32, CAP, 512), BF),
            pltpu.VMEM((16, CAP, 512), BF),
            pltpu.VMEM((128, 512), F32),
            dma((5,)), dma((7,)), dma((16,)), dma((2, 2)), dma((8, 4)), dma((2,)),
            dma((2, 5)), dma((2,)), dma((1,)), dma((2,)),
        ],
        compiler_params=pltpu.CompilerParams(
            collective_id=0, has_side_effects=True, vmem_limit_bytes=46000000
        ),
        name="handover",
    )(
        prompt,
        expert_ids.T.astype(F32),
        norm_gain.reshape(1, -1),
        gate_train.reshape(16, 2, 256, 128),
        up_train.reshape(16, 2, 256, 128),
        down_train.reshape(16, 2, 64, 512),
    )

    return pl.pallas_call(
        settle,
        out_shape=(
            jax.ShapeDtypeStruct((512, 512), BF),
            jax.ShapeDtypeStruct((2, 4096, 128), BF),
            jax.ShapeDtypeStruct((2, 4096, 128), BF),
            jax.ShapeDtypeStruct((2, 128, 4096), BF),
        ),
        in_specs=[any_ref] * 3 + [vmem_ref] * 5,
        out_specs=(hbm_ref,) * 4,
        scratch_shapes=[pltpu.VMEM((512, 512), BF), pltpu.VMEM((2, 512, 128), F32), dma((7,))],
        compiler_params=pltpu.CompilerParams(vmem_limit_bytes=6 << 20),
        name="settle",
    )(*made, group_weight.reshape(1, -1), expert_share.T)


def solution(mesh):
    placed = (
        P("fs", None),
        P("fs", None),
        P("fs"),
        P("fs", None),
        P("fs"),
        P(None, "fs", "tp"),
        P(None, "fs", "tp"),
        P(None, "fs", "tp"),
    )
    return jax.shard_map(
        on_device,
        mesh=mesh,
        in_specs=placed,
        out_specs=(P("fs", "tp"), P("fs", None, "tp"), P("fs", None, "tp"), P("fs", "tp", None)),
        check_vma=False,
    )
```

```python
import jax
import jax.numpy as jnp
from jax import lax
from jax.experimental import pallas as pl
from jax.experimental.pallas import tpu as pltpu
from jax.sharding import PartitionSpec as P

MESH = pl.DeviceIdType.MESH
BF = jnp.bfloat16
F32 = jnp.float32
EPS = 1e-06
CAP = 48
ORDER = (4, 12, 1, 3, 5, 15, 7, 13, 8, 2, 10, 6, 14, 9, 11)


def kernel(
    prompt, small, gate, up, down,
    gate_o, up_o, down_o, ret1, comb1, picked0,
    pf, xn, gb, sw, sd, wsend, dsend, cm, tsend, rows, drecv,
    hid, stage, ret0, cols,
    l_s, s_s, t_r, w_r, x_r, x_b, h_r, d_r, n_r, b_r,
):
    f = lax.axis_index("fs")
    t = lax.axis_index("tp")
    z, y = f // 4, f % 4
    x, c = t // 2, t % 2
    right = ((x + 1) % 4) * 2 + c
    left = ((x + 3) % 4) * 2 + c
    across = ((x + 2) % 4) * 2 + c
    mate = x * 2 + 1 - c
    flip = 1 - 2 * c

    def to(k):
        return ((z + k // 4) % 4) * 4 + (y + k % 4) % 4

    def came(k):
        return ((z + 4 - k // 4) % 4) * 4 + (y + 4 - k % 4) % 4

    def at(start, size, unit):
        return pl.ds(pl.multiple_of(start, unit), size)

    def local(src, dst, sem):
        return pltpu.make_async_copy(src, dst, sem)

    def remote(src, dst, ssem, rsem, fs, tp):
        return pltpu.make_async_remote_copy(
            src_ref=src, dst_ref=dst, send_sem=ssem, recv_sem=rsem,
            device_id=(fs, tp), device_id_type=MESH,
        )

    def arrived(ref, sem):
        remote(ref, ref, s_s.at[0], sem, f, mate).wait_recv()

    def sent(ref, sem):
        remote(ref, ref, sem, n_r.at[0], f, mate).wait_send()

    barrier = pltpu.get_barrier_semaphore()

    def greet_fs(k, carry):
        pl.semaphore_signal(barrier, inc=1, device_id=(to(k), t), device_id_type=MESH)
        return carry

    def greet_tp(k, carry):
        pl.semaphore_signal(barrier, inc=1, device_id=(f, (t + k) % 8), device_id_type=MESH)
        return carry

    lax.fori_loop(1, 16, greet_fs, 0)
    lax.fori_loop(1, 8, greet_tp, 0)

    for half_rows in range(2):
        block = pl.ds(half_rows * 256, 256)
        for i in range(16):
            local(
                prompt.at[block, i * 256 : (i + 1) * 256], pf.at[i, block, :], l_s.at[half_rows]
            ).start()

    chain = (0,) + ORDER
    source = (gate, up)
    fresh = (gate_o, up_o)
    ret = (ret0, ret1)
    comb = (pf, comb1)

    def load_weights(i, e, m, sem):
        return local(source[m].at[to(chain[(i + 1) % 16]), e], sw.at[i, m], l_s.at[sem])

    for i in range(8):
        load_weights(i, 0, 0, 5).start()
    for i in range(16):
        for m in range(2):
            if i > 7 or m:
                load_weights(i, 0, m, 2).start()

    ids = small.at[0:2]
    gb[...] = jnp.broadcast_to(small[2:3, 0:256], (128, 256)).T

    def rank_slots():
        expert = lax.broadcasted_iota(jnp.int32, (32, 512), 0).astype(F32)
        hit0 = ids[0:1, :] == expert
        hit1 = ids[1:2, :] == expert
        named = jnp.where(hit0 | hit1, 1.0, 0.0)
        before = jnp.where(
            lax.broadcasted_iota(jnp.int32, (512, 512), 0)
            < lax.broadcasted_iota(jnp.int32, (512, 512), 1), 1.0, 0.0,
        ).astype(BF)
        count = jnp.dot(named.astype(BF), before, preferred_element_type=F32)
        cm[...] = jnp.where(named > 0.5, count, -1.0)
        for k, hit in ((0, hit0), (1, hit1)):
            rank = jnp.sum(jnp.where(hit, count, 0.0), axis=0, keepdims=True)
            expert_of = ids[k : k + 1, :]
            pair = jnp.floor(expert_of * 0.5)
            place = (expert_of - 2.0 * pair) * 768.0 + pair * float(CAP)
            cols[k : k + 1, :] = place + rank

    cols[...] = jnp.zeros_like(cols)
    rank_slots()

    def build_pick(e, carry):
        slot = lax.broadcasted_iota(jnp.int32, (CAP, 512), 0).astype(F32)
        stage[e] = jnp.where(cm[pl.ds(e, 1), :] == slot, 1.0, 0.0).astype(BF)
        return carry

    lax.fori_loop(0, 32, build_pick, 0)

    def cast_weights(i, e, m):
        wsend[chain[(i + 1) % 16], e, m] = (sw[i, m] * gb[...]).astype(BF)

    def weights_copy(k, e, m):
        return remote(
            wsend.at[k, e, m], fresh[m].at[e, at(f * 256, 256, 256), :],
            s_s.at[0], w_r.at[e, m], to(k), t,
        )

    def normalize(i, carry):
        block = at(i * 32, 32, 32)
        squares = jnp.zeros((32, 256), F32)
        for j in range(16):
            part = pf[j, block, :].astype(F32)
            squares = squares + part * part
        mean = jnp.sum(squares, axis=1, keepdims=True) * (1.0 / 4096.0)
        scale = lax.rsqrt(mean + EPS)
        for h in range(2):
            part = pf[2 * t + h, block, :].astype(F32)
            xn[block, h * 256 : (h + 1) * 256] = (part * scale).astype(BF)
        return carry

    for half_rows in range(2):
        ready = pf.at[:, pl.ds(half_rows * 256, 256), :]
        local(ready, ready, l_s.at[half_rows]).wait()
        lax.fori_loop(half_rows * 8, half_rows * 8 + 8, normalize, 0, unroll=4)

    for g in range(4):
        chosen = stage[g * 8 : g * 8 + 8].reshape(384, 512)
        tsend[4 * g : 4 * g + 4] = (
            jnp.dot(chosen, xn[...], preferred_element_type=F32).astype(BF).reshape(4, 2, CAP, 512)
        )

    def token_copy(k, e):
        return remote(
            tsend.at[to(k), e], rows.at[t, e, at(f * CAP, CAP, CAP), :],
            s_s.at[1], t_r.at[k], to(k), t,
        )

    pl.semaphore_wait(barrier, 22)
    for near in (ORDER[:4], ORDER[4:8], ORDER[8:11], ORDER[11:]):
        for e in range(2):
            for k in near:
                token_copy(k, e).start()
    rows[t, :, at(f * CAP, CAP, CAP), :] = tsend[f]

    local(sw.at[pl.ds(0, 8), 0], sw.at[pl.ds(0, 8), 0], l_s.at[5]).wait()
    for i in range(8):
        cast_weights(i, 0, 0)
    for k in ORDER[:8]:
        weights_copy(k, 0, 0).start()
    local(sw.at[pl.ds(0, 12)], sw.at[pl.ds(0, 12)], l_s.at[2]).wait()
    for m in range(2):
        for i in range(16):
            if i > 7 or m:
                cast_weights(i, 0, m)
    for k in ORDER[8:]:
        weights_copy(k, 0, 0).start()
    for k in ORDER:
        weights_copy(k, 0, 1).start()
    for i in range(16):
        for m in range(2):
            load_weights(i, 1, m, 3).start()

    def load_down(i):
        return local(down.at[to(chain[i])], sd.at[pl.ds(i % 8 * 2, 2)], l_s.at[4])

    for i in range(8):
        load_down(i).start()

    def row_copy(k, n):
        r = at(came(k) * CAP, CAP, CAP)
        both = {0: (t, right), 1: (t, left), 2: (t, mate), 3: (left, mate), 5: (right, mate)}
        if n in both:
            s, who = both[n]
            ref = rows.at[s, :, r, :]
        else:
            s, e, who = {4: (left, 0, right), 6: (right, 1, left), 7: (across, 0, mate), 8: (across, 1, mate)}[n]
            ref = rows.at[s, e, r, :]
        slot = {0: 0, 1: 1, 4: 2, 6: 3}
        i = chain.index(k) // 2
        sem = x_r.at[i, slot[n]] if n in slot else x_b.at[n // 7]
        return remote(ref, ref, s_s.at[2], sem, f, who)

    pair = pl.ds(0, 2 * CAP)

    def token_round(part):
        for k in part:
            if k:
                arrived(tsend.at[0], t_r.at[k])
            for n in range(3):
                row_copy(k, n).start()

    token_round(chain[:6])
    local(sw, sw, l_s.at[3]).wait()
    for m in range(2):
        for i in range(16):
            cast_weights(i, 1, m)
        for k in ORDER:
            weights_copy(k, 1, m).start()
    for m in range(2):
        fresh[m][:, at(f * 256, 256, 256), :] = wsend[0, :, m]
    token_round(chain[6:])

    def down_copy(k, e):
        return remote(
            dsend.at[k, e], drecv.at[e, at(f * 64, 64, 64), :], s_s.at[3], d_r.at[e], to(k), t
        )

    def cast_down(base):
        local(sd, sd, l_s.at[4]).wait()
        for i in range(8):
            for e in range(2):
                dsend[chain[base + i], e] = sd[2 * i + e].astype(BF)

    def relay(i):
        arrived(rows.at[left, :, pair, :], x_r.at[i, 0])
        for k in chain[2 * i : 2 * i + 2]:
            row_copy(k, 4).start()
            row_copy(k, 3).start()
        arrived(rows.at[right, :, pair, :], x_r.at[i, 1])
        for k in chain[2 * i : 2 * i + 2]:
            row_copy(k, 6).start()
            row_copy(k, 5).start()

    cast_down(0)
    for i in range(8, 16):
        load_down(i).start()
    for i in range(3):
        relay(i)
    cast_down(8)
    drecv[:, at(f * 64, 64, 64), :] = dsend[0]
    for e in range(2):
        for k in ORDER:
            down_copy(k, e).start()
    for i in range(3, 6):
        relay(i)
    cols_t = cols[...].T
    lane = lax.broadcasted_iota(jnp.int32, (512, 256), 1).astype(F32)
    for k in range(2):
        for n in range(6):
            hit = cols_t[:, k : k + 1] == lane + 256.0 * n
            comb[n // 3][k * 3 + n % 3] = jnp.where(hit, 1.0, 0.0).astype(BF)
    for i in range(6, 8):
        relay(i)

    def project(e, chip):
        part = at(chip * 1024, 1024, 1024)
        left_side = jnp.concatenate([rows[2 * chip, e], rows[2 * chip + 1, e]], axis=1)
        both = jnp.concatenate([gate_o[e, part, :], up_o[e, part, :]], axis=1)
        return jnp.dot(left_side, both, preferred_element_type=F32)

    def total(e):
        return sd.at[pl.ds(0, 12), :, pl.ds(e * 256, 256)]

    def near(e):
        total(e)[...] = project(e, x).reshape(12, 64, 256)

        def step(j, carry):
            total(e)[...] += project(e, (x + j + j // 2) % 4).reshape(12, 64, 256)
            return carry

        lax.fori_loop(1, 3, step, 0)

    def finish(e):
        last = project(e, (x + 2) % 4) + total(e)[...].reshape(768, 256)
        v = last[:, 0:128]
        hid[t, e] = (v / (1.0 + jnp.exp(-v)) * last[:, 128:256]).astype(BF)

    def hidden_ref(s, e, part):
        return hid.at[s, e] if part is None else hid.at[s, e, pl.ds(part * 384, 384), :]

    def hidden_copy(e, n):
        s, part, who = (
            (t, None, right), (t, None, left), (t, None, mate), (left, None, mate), (left, 0, right),
            (right, None, mate), (right, 1, left), (across, 0, mate), (across, 1, mate),
        )[n]
        ref = hidden_ref(s, e, part)
        slot = {0: 0, 1: 1, 4: 2, 6: 3}.get(n, 4)
        return remote(ref, ref, s_s.at[4], h_r.at[e, slot], f, who)

    half = pl.ds(0, 384)

    for m in range(2):
        arrived(fresh[m].at[0, pl.ds(0, 3840), :], w_r.at[0, m])
    arrived(rows.at[pl.ds(0, 3)], x_b.at[0])
    near(0)
    for i in range(8):
        arrived(rows.at[across, 0, pair, :], x_r.at[i, 2])
        for k in chain[2 * i : 2 * i + 2]:
            row_copy(k, 7).start()
        arrived(rows.at[across, 1, pair, :], x_r.at[i, 3])
        for k in chain[2 * i : 2 * i + 2]:
            row_copy(k, 8).start()
    arrived(rows.at[0], x_b.at[1])
    finish(0)
    for n in range(3):
        hidden_copy(0, n).start()
    for m in range(2):
        arrived(fresh[m].at[1, pl.ds(0, 3840), :], w_r.at[1, m])
    near(1)
    finish(1)
    for n in range(3):
        hidden_copy(1, n).start()

    for e in range(2):
        arrived(hid.at[left, e], h_r.at[e, 0])
        hidden_copy(e, 4).start()
        hidden_copy(e, 3).start()
        arrived(hid.at[right, e], h_r.at[e, 1])
        hidden_copy(e, 6).start()
        hidden_copy(e, 5).start()

    def new_copy(k, e):
        s = (x + k // 2) % 4 * 2 + (c + k) % 2
        return remote(
            drecv.at[e, at(s * 128, 128, 128), :], down_o.at[e, :, at(t * 512, 512, 512)],
            s_s.at[5], n_r.at[0], f, s,
        )

    def back_copy(k, e):
        return remote(
            stage.at[e * 16 + to(k)], ret[e].at[f], s_s.at[6], b_r.at[e], to(k), t
        )

    for e in range(2):
        for n in range(2):
            arrived(hid.at[across, e, half, :], h_r.at[e, 2 + n])
            hidden_copy(e, 7 + n).start()
        arrived(drecv.at[e, pl.ds(0, 960), :], d_r.at[e])
        for k in (2, 6, 3, 7, 4, 5, 1):
            new_copy(k, e).start()
        arrived(hid.at[pl.ds(0, 4), e], h_r.at[e, 4])

        def expert_out(g, carry):
            part = at(g * 192, 192, 192)
            h = jnp.concatenate([hid[s, e, part, :] for s in range(8)], axis=1)
            out = jnp.dot(h, drecv[e], preferred_element_type=F32).astype(BF)
            stage[pl.ds(e * 16 + g * 4, 4)] = out.reshape(4, CAP, 512)
            return carry

        lax.fori_loop(0, 4, expert_out, 0)
        for k in ORDER:
            back_copy(k, e).start()
        ret[e][f] = stage[e * 16 + f]
        down_o[e, :, at(t * 512, 512, 512)] = drecv[e, at(t * 128, 128, 128), :]

    arrived(ret0.at[pl.ds(0, 15)], b_r.at[0])
    for k in range(2):
        picked0[k] = pick_rows(pf, ret0, k, pl.ds(0, 512)).astype(BF)
    arrived(down_o.at[:, :, pl.ds(0, 3584)], n_r.at[0])
    arrived(ret1.at[pl.ds(0, 15)], b_r.at[1])
    sent(wsend.at[pl.ds(0, 15)], s_s.at[0])
    sent(tsend.at[pl.ds(0, 15)], s_s.at[1])
    sent(rows.at[pl.ds(0, 7)], s_s.at[2])
    sent(dsend.at[pl.ds(0, 15)], s_s.at[3])
    sent(hid.at[pl.ds(0, 7)], s_s.at[4])
    sent(down_o.at[:, :, pl.ds(0, 3584)], s_s.at[5])
    sent(stage.at[pl.ds(0, 30)], s_s.at[6])


def pick_rows(comb, ret, k, part):
    picked = 0.0
    for n in range(3):
        back = ret[...].reshape(768, 512)[n * 256 : (n + 1) * 256]
        picked += jnp.dot(comb[k * 3 + n, part, :], back, preferred_element_type=F32)
    return picked


def settle(
    gate, up, down, ret1, comb1, picked0, gw, share,
    mixed_o, gate_o, up_o, down_o, mixed, weight, sem,
):
    moves = [
        pltpu.make_async_copy(src, dst, sem.at[n])
        for n, (src, dst) in enumerate(((gate, gate_o), (up, up_o), (down, down_o)))
    ]
    for move in moves:
        move.start()
    total = share[0:1, :] + share[1:2, :]
    for k in range(2):
        row = gw[...] * share[k : k + 1, :] / total
        weight[k] = jnp.broadcast_to(row, (128, 512)).T
    for n in range(4):
        part = pl.ds(n * 128, 128)
        sums = []
        for k in range(2):
            value = picked0[k, part, :].astype(F32) + pick_rows(comb1, ret1, k, part)
            sums.append(value * weight[k, part, 0:1])
        mixed[part, :] = (sums[0] + sums[1]).astype(BF)
        moves.append(pltpu.make_async_copy(mixed.at[part], mixed_o.at[part], sem.at[3 + n]))
        moves[-1].start()
    for move in moves:
        move.wait()


def on_device(
    prompt, expert_ids, group_weight, expert_share, norm_gain, gate_train, up_train, down_train
):
    any_ref = pl.BlockSpec(memory_space=pl.ANY)
    vmem_ref = pl.BlockSpec(memory_space=pltpu.VMEM)
    hbm_ref = pl.BlockSpec(memory_space=pltpu.HBM)
    dma = pltpu.SemaphoreType.DMA
    packed = lax.pad(expert_ids, 0, ((0, 0, 0), (0, 6, 0))).astype(F32) + lax.pad(
        norm_gain[:, None], 0.0, ((0, 256, 0), (2, 5, 0))
    )
    made = pl.pallas_call(
        kernel,
        out_shape=(
            jax.ShapeDtypeStruct((2, 4096, 128), BF),
            jax.ShapeDtypeStruct((2, 4096, 128), BF),
            jax.ShapeDtypeStruct((2, 128, 4096), BF),
            jax.ShapeDtypeStruct((16, CAP, 512), BF),
            jax.ShapeDtypeStruct((6, 512, 256), BF),
            jax.ShapeDtypeStruct((2, 512, 512), BF),
        ),
        in_specs=[hbm_ref, vmem_ref] + [hbm_ref] * 3,
        out_specs=(vmem_ref,) * 6,
        scratch_shapes=[
            pltpu.VMEM((16, 512, 256), BF),
            pltpu.VMEM((512, 512), BF),
            pltpu.VMEM((256, 128), F32),
            pltpu.VMEM((16, 2, 256, 128), F32),
            pltpu.VMEM((16, 64, 512), F32),
            pltpu.VMEM((16, 2, 2, 256, 128), BF),
            pltpu.VMEM((16, 2, 64, 512), BF),
            pltpu.VMEM((32, 512), F32),
            pltpu.VMEM((16, 2, CAP, 512), BF),
            pltpu.VMEM((8, 2, 768, 512), BF),
            pltpu.VMEM((2, 1024, 512), BF),
            pltpu.VMEM((8, 2, 768, 128), BF),
            pltpu.VMEM((32, CAP, 512), BF),
            pltpu.VMEM((16, CAP, 512), BF),
            pltpu.VMEM((128, 512), F32),
            dma((6,)), dma((7,)), dma((16,)), dma((2, 2)), dma((8, 4)), dma((2,)),
            dma((2, 5)), dma((2,)), dma((1,)), dma((2,)),
        ],
        compiler_params=pltpu.CompilerParams(
            collective_id=0, has_side_effects=True, vmem_limit_bytes=46000000
        ),
        name="handover",
    )(
        prompt,
        packed.T,
        gate_train.reshape(16, 2, 256, 128),
        up_train.reshape(16, 2, 256, 128),
        down_train.reshape(16, 2, 64, 512),
    )

    return pl.pallas_call(
        settle,
        out_shape=(
            jax.ShapeDtypeStruct((512, 512), BF),
            jax.ShapeDtypeStruct((2, 4096, 128), BF),
            jax.ShapeDtypeStruct((2, 4096, 128), BF),
            jax.ShapeDtypeStruct((2, 128, 4096), BF),
        ),
        in_specs=[any_ref] * 3 + [vmem_ref] * 5,
        out_specs=(hbm_ref,) * 4,
        scratch_shapes=[pltpu.VMEM((512, 512), BF), pltpu.VMEM((2, 512, 128), F32), dma((7,))],
        compiler_params=pltpu.CompilerParams(vmem_limit_bytes=6 << 20),
        name="settle",
    )(*made, group_weight.reshape(1, -1), expert_share.T)


def solution(mesh):
    placed = (
        P("fs", None),
        P("fs", None),
        P("fs"),
        P("fs", None),
        P("fs"),
        P(None, "fs", "tp"),
        P(None, "fs", "tp"),
        P(None, "fs", "tp"),
    )
    return jax.shard_map(
        on_device,
        mesh=mesh,
        in_specs=placed,
        out_specs=(P("fs", "tp"), P("fs", None, "tp"), P("fs", None, "tp"), P("fs", "tp", None)),
        check_vma=False,
    )
```

```python
import jax
import jax.numpy as jnp
from jax import lax
from jax.experimental import pallas as pl
from jax.experimental.pallas import tpu as pltpu
from jax.sharding import PartitionSpec as P

MESH = pl.DeviceIdType.MESH
BF = jnp.bfloat16
F32 = jnp.float32
EPS = 1e-06
CAP = 48
ORDER = (4, 12, 1, 3, 5, 15, 7, 13, 8, 2, 10, 6, 14, 9, 11)


def kernel(
    prompt, small, gate, up, down,
    gate_o, up_o, down_o, ret1, comb1, picked0,
    pf, po, xn, gb, sw, sd, wsend, dsend, cm, tsend, rows, drecv,
    hid, stage, ret0, cols,
    l_s, s_s, t_r, w_r, x_r, x_b, h_r, d_r, n_r, b_r,
):
    f = lax.axis_index("fs")
    t = lax.axis_index("tp")
    z, y = f // 4, f % 4
    x, c = t // 2, t % 2
    right = ((x + 1) % 4) * 2 + c
    left = ((x + 3) % 4) * 2 + c
    across = ((x + 2) % 4) * 2 + c
    mate = x * 2 + 1 - c
    flip = 1 - 2 * c

    def to(k):
        return ((z + k // 4) % 4) * 4 + (y + k % 4) % 4

    def came(k):
        return ((z + 4 - k // 4) % 4) * 4 + (y + 4 - k % 4) % 4

    def at(start, size, unit):
        return pl.ds(pl.multiple_of(start, unit), size)

    def local(src, dst, sem):
        return pltpu.make_async_copy(src, dst, sem)

    def remote(src, dst, ssem, rsem, fs, tp):
        return pltpu.make_async_remote_copy(
            src_ref=src, dst_ref=dst, send_sem=ssem, recv_sem=rsem,
            device_id=(fs, tp), device_id_type=MESH,
        )

    def arrived(ref, sem):
        remote(ref, ref, s_s.at[0], sem, f, mate).wait_recv()

    def sent(ref, sem):
        remote(ref, ref, sem, n_r.at[0], f, mate).wait_send()

    local(prompt.at[:, at(t * 512, 512, 512)], po, l_s.at[0]).start()
    for i in range(4):
        block = pl.ds(i * 128, 128)
        local(prompt.at[block, :], pf.at[block, :], l_s.at[i // 2]).start()

    barrier = pltpu.get_barrier_semaphore()

    def greet_fs(k, carry):
        pl.semaphore_signal(barrier, inc=1, device_id=(to(k), t), device_id_type=MESH)
        return carry

    def greet_tp(k, carry):
        pl.semaphore_signal(barrier, inc=1, device_id=(f, (t + k) % 8), device_id_type=MESH)
        return carry

    lax.fori_loop(1, 16, greet_fs, 0)
    lax.fori_loop(1, 8, greet_tp, 0)

    chain = (0,) + ORDER
    source = (gate, up)
    fresh = (gate_o, up_o)
    ret = (ret0, ret1)

    def load_weights(i, e, m, sem):
        return local(source[m].at[to(chain[(i + 1) % 16]), e], sw.at[i, m], l_s.at[sem])

    for i in range(8):
        load_weights(i, 0, 0, 5).start()
    for i in range(16):
        for m in range(2):
            if i > 7 or m:
                load_weights(i, 0, m, 2).start()

    ids = small.at[0:2]
    gb[...] = jnp.broadcast_to(small[2:3, 0:256], (128, 256)).T

    def rank_slots():
        expert = lax.broadcasted_iota(jnp.int32, (32, 512), 0).astype(F32)
        hit0 = ids[0:1, :] == expert
        hit1 = ids[1:2, :] == expert
        named = jnp.where(hit0 | hit1, 1.0, 0.0)
        before = jnp.where(
            lax.broadcasted_iota(jnp.int32, (512, 512), 0)
            < lax.broadcasted_iota(jnp.int32, (512, 512), 1), 1.0, 0.0,
        ).astype(BF)
        count = jnp.dot(named.astype(BF), before, preferred_element_type=F32)
        cm[...] = jnp.where(named > 0.5, count, -1.0)
        for k, hit in ((0, hit0), (1, hit1)):
            rank = jnp.sum(jnp.where(hit, count, 0.0), axis=0, keepdims=True)
            expert_of = ids[k : k + 1, :]
            pair = jnp.floor(expert_of * 0.5)
            place = (expert_of - 2.0 * pair) * 768.0 + pair * float(CAP)
            cols[k : k + 1, :] = place + rank

    cols[...] = jnp.zeros_like(cols)
    rank_slots()

    def build_pick(e, carry):
        slot = lax.broadcasted_iota(jnp.int32, (CAP, 512), 0).astype(F32)
        stage[e] = jnp.where(cm[pl.ds(e, 1), :] == slot, 1.0, 0.0).astype(BF)
        return carry

    lax.fori_loop(0, 32, build_pick, 0)

    def cast_weights(i, e, m):
        wsend[chain[(i + 1) % 16], e, m] = (sw[i, m] * gb[...]).astype(BF)

    def weights_copy(k, e, m):
        return remote(
            wsend.at[k, e, m], fresh[m].at[e, at(f * 256, 256, 256), :],
            s_s.at[0], w_r.at[e, m], to(k), t,
        )

    def normalize(i, carry):
        block = at(i * 32, 32, 32)
        squares = jnp.zeros((32, 256), F32)
        for j in range(16):
            part = pf[block, j * 256 : (j + 1) * 256].astype(F32)
            squares = squares + part * part
        mean = jnp.sum(squares, axis=1, keepdims=True) * (1.0 / 4096.0)
        xn[block, :] = (po[block, :].astype(F32) * lax.rsqrt(mean + EPS)).astype(BF)
        return carry

    for half_rows, size in ((0, 320), (1, 256)):
        ready = pf.at[pl.ds(0, size), :]
        local(ready, ready, l_s.at[half_rows]).wait()
        lax.fori_loop(half_rows * 8, half_rows * 8 + 8, normalize, 0, unroll=4)

    for g in range(4):
        chosen = stage[g * 8 : g * 8 + 8].reshape(384, 512)
        tsend[4 * g : 4 * g + 4] = (
            jnp.dot(chosen, xn[...], preferred_element_type=F32).astype(BF).reshape(4, 2, CAP, 512)
        )

    def token_copy(k, e):
        return remote(
            tsend.at[to(k), e], rows.at[t, e, at(f * CAP, CAP, CAP), :],
            s_s.at[1], t_r.at[k], to(k), t,
        )

    pl.semaphore_wait(barrier, 22)
    for near in (ORDER[:4], ORDER[4:8], ORDER[8:11], ORDER[11:]):
        for e in range(2):
            for k in near:
                token_copy(k, e).start()
    rows[t, :, at(f * CAP, CAP, CAP), :] = tsend[f]

    local(sw.at[pl.ds(0, 8), 0], sw.at[pl.ds(0, 8), 0], l_s.at[5]).wait()
    for i in range(8):
        cast_weights(i, 0, 0)
    for k in ORDER[:8]:
        weights_copy(k, 0, 0).start()
    local(sw.at[pl.ds(0, 12)], sw.at[pl.ds(0, 12)], l_s.at[2]).wait()
    for m in range(2):
        for i in range(16):
            if i > 7 or m:
                cast_weights(i, 0, m)
    for k in ORDER[8:]:
        weights_copy(k, 0, 0).start()
    for k in ORDER:
        weights_copy(k, 0, 1).start()
    for i in range(16):
        for m in range(2):
            load_weights(i, 1, m, 3).start()

    def load_down(i):
        return local(down.at[to(chain[i])], sd.at[pl.ds(i % 8 * 2, 2)], l_s.at[4])

    for i in range(8):
        load_down(i).start()

    def row_copy(k, n):
        r = at(came(k) * CAP, CAP, CAP)
        both = {0: (t, right), 1: (t, left), 2: (t, mate), 3: (left, mate), 5: (right, mate)}
        if n in both:
            s, who = both[n]
            ref = rows.at[s, :, r, :]
        else:
            s, e, who = {4: (left, 0, right), 6: (right, 1, left), 7: (across, 0, mate), 8: (across, 1, mate)}[n]
            ref = rows.at[s, e, r, :]
        slot = {0: 0, 1: 1, 4: 2, 6: 3}
        i = chain.index(k) // 2
        sem = x_r.at[i, slot[n]] if n in slot else x_b.at[n // 7]
        return remote(ref, ref, s_s.at[2], sem, f, who)

    pair = pl.ds(0, 2 * CAP)

    def token_round(part):
        for k in part:
            if k:
                arrived(tsend.at[0], t_r.at[k])
            for n in range(3):
                row_copy(k, n).start()

    token_round(chain[:6])
    local(sw, sw, l_s.at[3]).wait()
    for m in range(2):
        for i in range(16):
            cast_weights(i, 1, m)
        for k in ORDER:
            weights_copy(k, 1, m).start()
    for m in range(2):
        fresh[m][:, at(f * 256, 256, 256), :] = wsend[0, :, m]
    token_round(chain[6:])

    def down_copy(k, e):
        return remote(
            dsend.at[k, e], drecv.at[e, at(f * 64, 64, 64), :], s_s.at[3], d_r.at[e], to(k), t
        )

    def cast_down(base):
        local(sd, sd, l_s.at[4]).wait()
        for i in range(8):
            for e in range(2):
                dsend[chain[base + i], e] = sd[2 * i + e].astype(BF)

    def relay(i):
        arrived(rows.at[left, :, pair, :], x_r.at[i, 0])
        for k in chain[2 * i : 2 * i + 2]:
            row_copy(k, 4).start()
            row_copy(k, 3).start()
        arrived(rows.at[right, :, pair, :], x_r.at[i, 1])
        for k in chain[2 * i : 2 * i + 2]:
            row_copy(k, 6).start()
            row_copy(k, 5).start()

    cast_down(0)
    for i in range(8, 16):
        load_down(i).start()
    for i in range(3):
        relay(i)
    cast_down(8)
    drecv[:, at(f * 64, 64, 64), :] = dsend[0]
    for e in range(2):
        for k in ORDER:
            down_copy(k, e).start()
    for i in range(3, 6):
        relay(i)
    cols_t = cols[...].T
    lane = lax.broadcasted_iota(jnp.int32, (512, 256), 1).astype(F32)
    for k in range(2):
        for n in range(6):
            hit = cols_t[:, k : k + 1] == lane + 256.0 * n
            chosen = jnp.where(hit, 1.0, 0.0).astype(BF)
            if n < 3:
                pf[:, (k * 3 + n) * 256 : (k * 3 + n + 1) * 256] = chosen
            else:
                comb1[k * 3 + n - 3] = chosen
    for i in range(6, 8):
        relay(i)

    def project(e, chip):
        part = at(chip * 1024, 1024, 1024)
        left_side = jnp.concatenate([rows[2 * chip, e], rows[2 * chip + 1, e]], axis=1)
        both = jnp.concatenate([gate_o[e, part, :], up_o[e, part, :]], axis=1)
        return jnp.dot(left_side, both, preferred_element_type=F32)

    def total(e):
        return sd.at[pl.ds(0, 12), :, pl.ds(e * 256, 256)]

    def near(e):
        total(e)[...] = project(e, x).reshape(12, 64, 256)

        def step(j, carry):
            total(e)[...] += project(e, (x + j + j // 2) % 4).reshape(12, 64, 256)
            return carry

        lax.fori_loop(1, 3, step, 0)

    def finish(e):
        last = project(e, (x + 2) % 4) + total(e)[...].reshape(768, 256)
        v = last[:, 0:128]
        hid[t, e] = (v / (1.0 + jnp.exp(-v)) * last[:, 128:256]).astype(BF)

    def hidden_ref(s, e, part):
        return hid.at[s, e] if part is None else hid.at[s, e, pl.ds(part * 384, 384), :]

    def hidden_copy(e, n):
        s, part, who = (
            (t, None, right), (t, None, left), (t, None, mate), (left, None, mate), (left, 0, right),
            (right, None, mate), (right, 1, left), (across, 0, mate), (across, 1, mate),
        )[n]
        ref = hidden_ref(s, e, part)
        slot = {0: 0, 1: 1, 4: 2, 6: 3}.get(n, 4)
        return remote(ref, ref, s_s.at[4], h_r.at[e, slot], f, who)

    half = pl.ds(0, 384)

    for m in range(2):
        arrived(fresh[m].at[0, pl.ds(0, 3840), :], w_r.at[0, m])
    arrived(rows.at[pl.ds(0, 3)], x_b.at[0])
    near(0)
    for i in range(8):
        arrived(rows.at[across, 0, pair, :], x_r.at[i, 2])
        for k in chain[2 * i : 2 * i + 2]:
            row_copy(k, 7).start()
        arrived(rows.at[across, 1, pair, :], x_r.at[i, 3])
        for k in chain[2 * i : 2 * i + 2]:
            row_copy(k, 8).start()
    arrived(rows.at[0], x_b.at[1])
    finish(0)
    for n in range(3):
        hidden_copy(0, n).start()
    for m in range(2):
        arrived(fresh[m].at[1, pl.ds(0, 3840), :], w_r.at[1, m])
    near(1)
    finish(1)
    for n in range(3):
        hidden_copy(1, n).start()

    for e in range(2):
        arrived(hid.at[left, e], h_r.at[e, 0])
        hidden_copy(e, 4).start()
        hidden_copy(e, 3).start()
        arrived(hid.at[right, e], h_r.at[e, 1])
        hidden_copy(e, 6).start()
        hidden_copy(e, 5).start()

    def new_copy(k, e):
        s = (x + k // 2) % 4 * 2 + (c + k) % 2
        return remote(
            drecv.at[e, at(s * 128, 128, 128), :], down_o.at[e, :, at(t * 512, 512, 512)],
            s_s.at[5], n_r.at[0], f, s,
        )

    def back_copy(k, e):
        return remote(
            stage.at[e * 16 + to(k)], ret[e].at[f], s_s.at[6], b_r.at[e], to(k), t
        )

    for e in range(2):
        for n in range(2):
            arrived(hid.at[across, e, half, :], h_r.at[e, 2 + n])
            hidden_copy(e, 7 + n).start()
        arrived(drecv.at[e, pl.ds(0, 960), :], d_r.at[e])
        for k in (2, 6, 3, 7, 4, 5, 1):
            new_copy(k, e).start()
        arrived(hid.at[pl.ds(0, 4), e], h_r.at[e, 4])

        def expert_out(g, carry):
            part = at(g * 192, 192, 192)
            h = jnp.concatenate([hid[s, e, part, :] for s in range(8)], axis=1)
            out = jnp.dot(h, drecv[e], preferred_element_type=F32).astype(BF)
            stage[pl.ds(e * 16 + g * 4, 4)] = out.reshape(4, CAP, 512)
            return carry

        lax.fori_loop(0, 4, expert_out, 0)
        for k in ORDER:
            back_copy(k, e).start()
        ret[e][f] = stage[e * 16 + f]
        down_o[e, :, at(t * 512, 512, 512)] = drecv[e, at(t * 128, 128, 128), :]

    arrived(ret0.at[pl.ds(0, 15)], b_r.at[0])
    for k in range(2):
        blocks = [pf[:, (k * 3 + n) * 256 : (k * 3 + n + 1) * 256] for n in range(3)]
        picked0[k] = pick_rows(blocks, ret0).astype(BF)
    arrived(down_o.at[:, :, pl.ds(0, 3584)], n_r.at[0])
    arrived(ret1.at[pl.ds(0, 15)], b_r.at[1])
    sent(wsend.at[pl.ds(0, 15)], s_s.at[0])
    sent(tsend.at[pl.ds(0, 15)], s_s.at[1])
    sent(rows.at[pl.ds(0, 7)], s_s.at[2])
    sent(dsend.at[pl.ds(0, 15)], s_s.at[3])
    sent(hid.at[pl.ds(0, 7)], s_s.at[4])
    sent(down_o.at[:, :, pl.ds(0, 3584)], s_s.at[5])
    sent(stage.at[pl.ds(0, 30)], s_s.at[6])


def pick_rows(blocks, ret):
    picked = 0.0
    for n in range(3):
        back = ret[...].reshape(768, 512)[n * 256 : (n + 1) * 256]
        picked += jnp.dot(blocks[n], back, preferred_element_type=F32)
    return picked


def settle(
    gate, up, down, ret1, comb1, picked0, gw, share,
    mixed_o, gate_o, up_o, down_o, mixed, weight, sem,
):
    moves = [
        pltpu.make_async_copy(src, dst, sem.at[n])
        for n, (src, dst) in enumerate(((gate, gate_o), (up, up_o), (down, down_o)))
    ]
    for move in moves:
        move.start()
    total = share[0:1, :] + share[1:2, :]
    for k in range(2):
        row = gw[...] * share[k : k + 1, :] / total
        weight[k] = jnp.broadcast_to(row, (128, 512)).T
    for n in range(4):
        part = pl.ds(n * 128, 128)
        sums = []
        for k in range(2):
            blocks = [comb1[k * 3 + m, part, :] for m in range(3)]
            value = picked0[k, part, :].astype(F32) + pick_rows(blocks, ret1)
            sums.append(value * weight[k, part, 0:1])
        mixed[part, :] = (sums[0] + sums[1]).astype(BF)
        moves.append(pltpu.make_async_copy(mixed.at[part], mixed_o.at[part], sem.at[3 + n]))
        moves[-1].start()
    for move in moves:
        move.wait()


def on_device(
    prompt, expert_ids, group_weight, expert_share, norm_gain, gate_train, up_train, down_train
):
    any_ref = pl.BlockSpec(memory_space=pl.ANY)
    vmem_ref = pl.BlockSpec(memory_space=pltpu.VMEM)
    hbm_ref = pl.BlockSpec(memory_space=pltpu.HBM)
    dma = pltpu.SemaphoreType.DMA
    packed = lax.pad(expert_ids, 0, ((0, 0, 0), (0, 6, 0))).astype(F32) + lax.pad(
        norm_gain[:, None], 0.0, ((0, 256, 0), (2, 5, 0))
    )
    made = pl.pallas_call(
        kernel,
        out_shape=(
            jax.ShapeDtypeStruct((2, 4096, 128), BF),
            jax.ShapeDtypeStruct((2, 4096, 128), BF),
            jax.ShapeDtypeStruct((2, 128, 4096), BF),
            jax.ShapeDtypeStruct((16, CAP, 512), BF),
            jax.ShapeDtypeStruct((6, 512, 256), BF),
            jax.ShapeDtypeStruct((2, 512, 512), BF),
        ),
        in_specs=[hbm_ref, vmem_ref] + [hbm_ref] * 3,
        out_specs=(vmem_ref,) * 6,
        scratch_shapes=[
            pltpu.VMEM((512, 4096), BF),
            pltpu.VMEM((512, 512), BF),
            pltpu.VMEM((512, 512), BF),
            pltpu.VMEM((256, 128), F32),
            pltpu.VMEM((16, 2, 256, 128), F32),
            pltpu.VMEM((16, 64, 512), F32),
            pltpu.VMEM((16, 2, 2, 256, 128), BF),
            pltpu.VMEM((16, 2, 64, 512), BF),
            pltpu.VMEM((32, 512), F32),
            pltpu.VMEM((16, 2, CAP, 512), BF),
            pltpu.VMEM((8, 2, 768, 512), BF),
            pltpu.VMEM((2, 1024, 512), BF),
            pltpu.VMEM((8, 2, 768, 128), BF),
            pltpu.VMEM((32, CAP, 512), BF),
            pltpu.VMEM((16, CAP, 512), BF),
            pltpu.VMEM((128, 512), F32),
            dma((6,)), dma((7,)), dma((16,)), dma((2, 2)), dma((8, 4)), dma((2,)),
            dma((2, 5)), dma((2,)), dma((1,)), dma((2,)),
        ],
        compiler_params=pltpu.CompilerParams(
            collective_id=0, has_side_effects=True, vmem_limit_bytes=46000000
        ),
        name="handover",
    )(
        prompt,
        packed.T,
        gate_train.reshape(16, 2, 256, 128),
        up_train.reshape(16, 2, 256, 128),
        down_train.reshape(16, 2, 64, 512),
    )

    return pl.pallas_call(
        settle,
        out_shape=(
            jax.ShapeDtypeStruct((512, 512), BF),
            jax.ShapeDtypeStruct((2, 4096, 128), BF),
            jax.ShapeDtypeStruct((2, 4096, 128), BF),
            jax.ShapeDtypeStruct((2, 128, 4096), BF),
        ),
        in_specs=[any_ref] * 3 + [vmem_ref] * 5,
        out_specs=(hbm_ref,) * 4,
        scratch_shapes=[pltpu.VMEM((512, 512), BF), pltpu.VMEM((2, 512, 128), F32), dma((7,))],
        compiler_params=pltpu.CompilerParams(vmem_limit_bytes=6 << 20),
        name="settle",
    )(*made, group_weight.reshape(1, -1), expert_share.T)


def solution(mesh):
    placed = (
        P("fs", None),
        P("fs", None),
        P("fs"),
        P("fs", None),
        P("fs"),
        P(None, "fs", "tp"),
        P(None, "fs", "tp"),
        P(None, "fs", "tp"),
    )
    return jax.shard_map(
        on_device,
        mesh=mesh,
        in_specs=placed,
        out_specs=(P("fs", "tp"), P("fs", None, "tp"), P("fs", None, "tp"), P("fs", "tp", None)),
        check_vma=False,
    )
```
